32 devices in a mesh: ep: 8 (over z, x), tp: 4 (over y, core).
Axes of the slice: x: 2, y: 2, z: 4, core: 2. Of those that a mesh axis runs over, the one named last changes fastest.
Arguments:
- mixer_query: bfloat16 [2048, 2048], P('ep', 'tp'), may hold values from -6 to 6
- mixer_forget: bfloat16 [2048, 2048], P('ep', 'tp'), may hold values from -5.5 to 5.5
- mixer_value: bfloat16 [2048, 2048], P('ep', 'tp'), may hold values from -6 to 6
- mixer_gate: bfloat16 [2048, 2048], P('ep', 'tp'), may hold values from -6 to 6
- forget_floor: float32 [2048], P('tp'), may hold values from 0.88 to 1
- head_gain: float32 [128], replicated, may hold values from 0.1 to 1.9
- mixer_proj: bfloat16 [2048, 2048], P(None, 'tp'), may hold values from -0.125 to 0.125
- expert_tokens: bfloat16 [1024, 2048], P('ep'), may hold values from -6 to 6
- expert_gain: float32 [2048], replicated, may hold values from 0.1 to 1.9
- routes: int32 [1024, 2], P('ep'), may hold values from 0 to 7, as said below
- group_logits: float32 [1024, 4], P('ep'), may hold values from -6 to 6
- choice_logits: float32 [1024, 2], P('ep'), may hold values from -6 to 6
- w_gate: bfloat16 [8, 2048, 2048], P('ep', None, 'tp'), may hold values from -0.125 to 0.125
- w_up: bfloat16 [8, 2048, 2048], P('ep', None, 'tp'), may hold values from -0.125 to 0.125
- w_down: bfloat16 [8, 2048, 2048], P('ep', None, 'tp'), may hold values from -0.125 to 0.125
Outputs:
- mixer_out: bfloat16 [2048, 2048], P('ep', 'tp')
- expert_out: bfloat16 [1024, 2048], P('ep', 'tp')
The draws below stay inside these ranges and needn't reach their ends.
Inputs may be any that keep to these rules, and one draw needn't show every extreme that they name: `routes`: in each aligned block of 128 rows (the rows of one index of ep) no expert is named by more than 64 rows, and some expert reaches that bound in every block; the 2 experts of a row differ and lie in the same group.
All inputs are finite; a program needn't handle non-finite values.
Results may differ from the reference program's by a relative error of at most 0.01.
Values may be sent and summed in bfloat16 or wider, within the bound.
A program may use at most 64 MiB of HBM per device.

```python
import math
import jax
import jax.numpy as jnp
from jax import lax

D = 2048
HEADS = 16
KEYDIM = 128
VDIM = 128
FF = 2048
GROUPS = 4
TOPK = 2
BLOCK = 64
TOKA_DEV = 256
TOKB_DEV = 128
EXPERTS = 8
EXP_GROUP = 2
CAP = 64
TOKENS_A = 2048
TOKENS_B = 1024
N_EP = 8


def draw_mixer_forget(key, part):
    noise_key = jax.random.fold_in(key, 11)
    shift_key = jax.random.fold_in(key, 12)
    noise = jnp.clip(jax.random.normal(noise_key, (TOKENS_A, HEADS * KEYDIM), jnp.float32), -4.0, 4.0)
    shifts = jax.random.uniform(shift_key, (TOKENS_A // TOKA_DEV, 1, 1), jnp.float32, -1.5, 1.5)
    shaped = noise.reshape(TOKENS_A // TOKA_DEV, TOKA_DEV, HEADS * KEYDIM) + shifts
    return shaped.reshape(TOKENS_A, HEADS * KEYDIM).astype(jnp.bfloat16)


def draw_forget_floor(key, part):
    pick_key = jax.random.fold_in(key, 21)
    slow_key = jax.random.fold_in(key, 22)
    fast_key = jax.random.fold_in(key, 23)
    slow_share = 0.5
    slow_heads = jax.random.uniform(pick_key, (HEADS, 1), jnp.float32) < slow_share
    slow_gap = jax.random.uniform(slow_key, (HEADS, KEYDIM), jnp.float32, 0.3, 2.0) / TOKENS_A
    fast_gap = jnp.exp(jax.random.uniform(fast_key, (HEADS, KEYDIM), jnp.float32, math.log(0.03), math.log(0.12)))
    gap_rows = jnp.where(slow_heads, slow_gap, fast_gap)
    return (1.0 - gap_rows).reshape(HEADS * KEYDIM).astype(jnp.float32)


def route_block(block_key):
    group_size = EXPERTS // GROUPS
    quota = TOKB_DEV // EXPERTS
    expert_ids = jnp.arange(EXPERTS, dtype=jnp.int32)
    counts = jnp.full((EXPERTS,), quota, jnp.int32)
    counts = counts + quota * ((expert_ids == 0) | (expert_ids == group_size - 1)).astype(jnp.int32)
    counts = counts - quota * ((expert_ids == group_size) | (expert_ids == group_size + 1)).astype(jnp.int32)
    canonical = jnp.repeat(expert_ids, counts, total_repeat_length=TOKB_DEV)
    order = jax.random.permutation(jax.random.fold_in(block_key, 1), TOKB_DEV)
    first = canonical[order]
    second = first // group_size * group_size + (first % group_size + 1) % group_size
    group_map = jax.random.permutation(jax.random.fold_in(block_key, 2), GROUPS).astype(jnp.int32)
    rotation = jax.random.randint(jax.random.fold_in(block_key, 3), (GROUPS,), 0, group_size).astype(jnp.int32)

    def relabel(ids):
        grp = ids // group_size
        return (group_map[grp] * group_size + (ids % group_size + rotation[grp]) % group_size).astype(jnp.int32)
    first = relabel(first)
    second = relabel(second)
    flip = jax.random.randint(jax.random.fold_in(block_key, 4), (TOKB_DEV,), 0, 2).astype(jnp.int32)
    left = flip * second + (1 - flip) * first
    right = flip * first + (1 - flip) * second
    return jnp.stack([left, right], axis=-1).astype(jnp.int32)


def draw_routes(key, part):
    base_key = jax.random.fold_in(key, 31)
    block_keys = jax.vmap(lambda index: jax.random.fold_in(base_key, index))(jnp.arange(N_EP))
    return jax.vmap(route_block)(block_keys).reshape(TOKENS_B, TOPK).astype(jnp.int32)


def steps_of(key, extent, cuts, least, largest):
    gain, own = 1.0, jax.random.fold_in(key, 6)
    for position, blocks in cuts:
        steps = jnp.exp(jax.random.uniform(jax.random.fold_in(own, position), (blocks,), jnp.float32, least / len(cuts), largest / len(cuts)))
        gain = gain * jnp.repeat(steps, extent[position] // blocks).reshape([-1 if axis == position else 1 for axis in range(len(extent))])
    return gain


def bell_draw(rng, shape, scale, bound, cuts=(), kind=jnp.bfloat16):
    loudness = steps_of(rng, shape, cuts, -0.22, 0.18) if cuts else 1.0
    values = jax.random.normal(rng, shape, jnp.float32) * scale * loudness
    return jnp.minimum(jnp.maximum(values, -bound), bound).astype(kind)


def setup_inputs(seed: int = 0) -> dict:
    key_of = jax.random.split(jax.random.key(seed), 16)
    return {
        "mixer_query": bell_draw(key_of[0], (TOKENS_A, HEADS * KEYDIM), 1.0, 6.0, ((0, 8), (1, 4))),
        "mixer_forget": draw_mixer_forget(jax.random.fold_in(key_of[15], 71), 0),
        "mixer_value": bell_draw(key_of[2], (TOKENS_A, HEADS * VDIM), 1.0, 6.0, ((0, 8), (1, 4))),
        "mixer_gate": bell_draw(key_of[3], (TOKENS_A, HEADS * VDIM), 1.0, 6.0, ((0, 8), (1, 4))),
        "forget_floor": draw_forget_floor(jax.random.fold_in(key_of[15], 71), 0),
        "head_gain": jnp.clip(1.0 + 0.18 * jax.random.normal(key_of[5], (VDIM,), jnp.float32), 0.1, 1.9),
        "mixer_proj": bell_draw(key_of[6], (HEADS * VDIM, D), (HEADS * VDIM) ** -0.5, 0.125, ((1, 4),)),
        "expert_tokens": bell_draw(key_of[7], (TOKENS_B, D), 1.0, 6.0, ((0, 8),)),
        "expert_gain": jnp.clip(1.0 + 0.18 * jax.random.normal(key_of[8], (D,), jnp.float32), 0.1, 1.9),
        "routes": draw_routes(jax.random.fold_in(key_of[15], 71), 0),
        "group_logits": bell_draw(key_of[10], (TOKENS_B, GROUPS), 1.0, 6.0, ((0, 8),), jnp.float32),
        "choice_logits": bell_draw(key_of[11], (TOKENS_B, TOPK), 1.0, 6.0, ((0, 8),), jnp.float32),
        "w_gate": bell_draw(key_of[12], (EXPERTS, D, FF), D ** -0.5, 0.125, ((0, 8), (2, 4))),
        "w_up": bell_draw(key_of[13], (EXPERTS, D, FF), D ** -0.5, 0.125, ((0, 8), (2, 4))),
        "w_down": bell_draw(key_of[14], (EXPERTS, FF, D), FF ** -0.5, 0.125, ((0, 8), (2, 4))),
    }


norm_eps = 1e-06
highest_precision = lax.Precision.HIGHEST

def rms_scale(features, gain_vec):
    return features * lax.rsqrt(lax.optimization_barrier(jnp.mean(features * features, axis=-1, keepdims=True)) + norm_eps) * gain_vec

def block_terms(query_block, input_block, log_blk, value_block, carried_state):
    cumulative_log = jnp.cumsum(log_blk, axis=0)
    between_block_term = jnp.einsum('zug,ugr->zur', query_block * jnp.exp(cumulative_log), carried_state, precision=highest_precision)
    causal = jnp.tril(jnp.ones((query_block.shape[0], query_block.shape[0]), dtype=bool))[:, :, None, None]
    differ = cumulative_log[:, None] - cumulative_log[None, :]
    decays = jnp.exp(jnp.where(causal, differ, -jnp.inf))
    scores = lax.optimization_barrier(jnp.sum(query_block[:, None] * input_block[None, :] * decays, axis=-1))
    result = between_block_term + jnp.einsum('tsh,shv->thv', scores, value_block, precision=highest_precision)
    ending_log_decay = cumulative_log[-1]
    updated_state = jnp.exp(ending_log_decay)[..., None] * carried_state + jnp.einsum('twa,twr->war', input_block * jnp.exp(ending_log_decay[None] - cumulative_log), value_block, precision=highest_precision)
    return (updated_state, result, cumulative_log)

def mixer_part(mixer_query, mixer_forget, mixer_value, mixer_gate, forget_floor, head_gain, mixer_proj):
    length = mixer_query.shape[0]
    blocks = length // BLOCK

    def split_blocks(source_array, last_width):
        return source_array.reshape(blocks, BLOCK, HEADS, last_width)
    queries = jax.nn.silu(mixer_query.astype(jnp.float32))
    input_rates = (1.0 - forget_floor) * jax.nn.sigmoid(-mixer_forget.astype(jnp.float32))
    log_forget = jnp.log1p(-input_rates)
    value_rows = mixer_value.astype(jnp.float32)

    def advance(carried_state, block_inputs):
        query_block, input_block, value_block, log_blk = block_inputs
        updated_state, result, cumulative_log = block_terms(query_block, input_block, log_blk, value_block, carried_state)
        return (updated_state, result)
    initial = jnp.zeros((HEADS, KEYDIM, VDIM), jnp.float32)
    _, output_rows = lax.scan(advance, initial, (split_blocks(queries, KEYDIM), split_blocks(input_rates, KEYDIM), split_blocks(value_rows, VDIM), split_blocks(log_forget, KEYDIM)))
    output_rows = output_rows.reshape(length, HEADS, VDIM)
    gate_act = jax.nn.silu(mixer_gate.astype(jnp.float32)).reshape(length, HEADS, VDIM)
    gated_out = rms_scale(output_rows, head_gain) * gate_act
    mixed_heads = gated_out.reshape(length, HEADS * VDIM).astype(jnp.bfloat16)
    return jnp.dot(mixed_heads, mixer_proj, preferred_element_type=jnp.float32).astype(jnp.bfloat16)

def gate_weights(routes, group_logits, choice_logits, group_size):
    group_exp = jnp.exp(group_logits)
    group_prob = group_exp / lax.optimization_barrier(jnp.sum(group_exp, axis=-1, keepdims=True))
    groups_of = routes // group_size
    member = (groups_of[..., None] == jnp.arange(GROUPS, dtype=jnp.int32)).astype(jnp.float32)
    picked_prob = lax.optimization_barrier(jnp.sum(member * group_prob[:, None, :], axis=-1))
    choice_exp = jnp.exp(choice_logits)
    together = (groups_of[:, :, None] == groups_of[:, None, :]).astype(jnp.float32)
    within = lax.optimization_barrier(jnp.sum(together * choice_exp[:, None, :], axis=-1))
    return picked_prob * choice_exp / within

def rank_slots(flat_routes, per_block, expert_count):
    onehot = (flat_routes[:, None] == jnp.arange(expert_count, dtype=jnp.int32)).astype(jnp.int32)
    blocked = onehot.reshape(-1, per_block, expert_count)
    earlier = (jnp.cumsum(blocked, axis=1) - blocked).astype(jnp.int32)
    return lax.optimization_barrier(jnp.sum(earlier * blocked, axis=-1)).astype(jnp.int32).reshape(-1)

def expert_part(expert_tokens, expert_gain, routes, group_logits, choice_logits, w_gate, w_up, w_down):
    count_rows = expert_tokens.shape[0]
    normed = rms_scale(expert_tokens.astype(jnp.float32), expert_gain).astype(jnp.bfloat16)
    weights = gate_weights(routes, group_logits, choice_logits, EXP_GROUP)
    flat_routes = routes.reshape(-1)
    per_block = TOKB_DEV * TOPK
    ranks = rank_slots(flat_routes, per_block, EXPERTS)
    block_ids = (jnp.arange(flat_routes.shape[0], dtype=jnp.int32) // per_block).astype(jnp.int32)
    slot_of = (flat_routes * (N_EP * CAP) + block_ids * CAP + ranks).astype(jnp.int32)
    token_ids = (jnp.arange(flat_routes.shape[0], dtype=jnp.int32) // TOPK).astype(jnp.int32)
    token_of = jnp.full((EXPERTS * N_EP * CAP,), count_rows, jnp.int32).at[slot_of].set(token_ids)
    padded = jnp.concatenate([normed, jnp.zeros((1, D), jnp.bfloat16)], axis=0)

    def run_expert(operands):
        gate_mat, up_mat, down_mat, index_rows = operands
        chosen = padded[index_rows]
        gate_pre = jnp.dot(chosen, gate_mat, preferred_element_type=jnp.float32)
        up_pre = jnp.dot(chosen, up_mat, preferred_element_type=jnp.float32)
        hidden = (jax.nn.silu(gate_pre) * up_pre).astype(jnp.bfloat16)
        return jnp.dot(hidden, down_mat, preferred_element_type=jnp.float32).astype(jnp.bfloat16)
    output_rows = lax.map(run_expert, (w_gate, w_up, w_down, token_of.reshape(EXPERTS, N_EP * CAP)))
    picked = output_rows.reshape(-1, D)[slot_of].astype(jnp.float32) * weights.reshape(-1)[:, None]
    return lax.optimization_barrier(jnp.sum(picked.reshape(count_rows, TOPK, D), axis=1)).astype(jnp.bfloat16)

def reference(mixer_query, mixer_forget, mixer_value, mixer_gate, forget_floor, head_gain, mixer_proj, expert_tokens, expert_gain, routes, group_logits, choice_logits, w_gate, w_up, w_down):
    mixer_out = mixer_part(mixer_query, mixer_forget, mixer_value, mixer_gate, forget_floor, head_gain, mixer_proj)
    expert_out = expert_part(expert_tokens, expert_gain, routes, group_logits, choice_logits, w_gate, w_up, w_down)
    return (mixer_out, expert_out)
```

```python
import jax
import jax.numpy as jnp
from jax import lax
from jax.experimental import pallas as pl
from jax.experimental.pallas import tpu as pltpu
from jax.sharding import PartitionSpec as P

KEYDIM = 128
VDIM = 128
GROUPS = 4
TOPK = 2
PAD = 16
norm_eps = 1e-06
F32 = jnp.float32
BF16 = jnp.bfloat16
VM = pl.BlockSpec(memory_space=pltpu.VMEM)
SM = pl.BlockSpec(memory_space=pltpu.SMEM)


def tn_dot(a, b):
    return lax.dot_general(a, b, (((0,), (0,)), ((), ())), preferred_element_type=F32)


def nt_dot(a, b):
    return lax.dot_general(a, b, (((1,), (1,)), ((), ())), preferred_element_type=F32)


def silu(v):
    return v / (1.0 + jnp.exp(-v))


def local_kernel(q_ref, f_ref, v_ref, floor_ref, intra_ref, qexp_ref, pay_ref):
    length = q_ref.shape[0]
    rows = lax.broadcasted_iota(jnp.int32, (length, length), 0)
    cols = lax.broadcasted_iota(jnp.int32, (length, length), 1)
    causal = cols <= rows
    tril = causal.astype(F32)
    for h in range(q_ref.shape[1] // KEYDIM):
        at = slice(h * KEYDIM, (h + 1) * KEYDIM)
        floor = floor_ref[:, at]
        rates = (1.0 - floor) / (1.0 + jnp.exp(f_ref[:, at].astype(F32)))
        cum = jnp.dot(
            tril, jnp.log(1.0 - rates), precision=lax.Precision.HIGHEST,
            preferred_element_type=F32,
        )
        end = cum[length - 1 : length, :]
        qexp = (silu(q_ref[:, at].astype(F32)) * jnp.exp(cum)).astype(BF16)
        kexp = (rates * jnp.exp(-cum)).astype(BF16)
        kend = (rates * jnp.exp(end - cum)).astype(BF16)
        value = v_ref[:, at]
        scores = jnp.where(causal, nt_dot(qexp, kexp), 0.0).astype(BF16)
        intra_ref[:, at] = jnp.dot(scores, value, preferred_element_type=F32)
        qexp_ref[:, at] = qexp
        pay_ref[h, :VDIM, :] = tn_dot(value, kend).astype(BF16)
        pay_ref[h, VDIM:, :] = jnp.broadcast_to(jnp.exp(end), (PAD, KEYDIM)).astype(BF16)


def finish_kernel(state_ref, intra_ref, qexp_ref, gate_ref, gain_ref, out_ref):
    for h in range(intra_ref.shape[1] // VDIM):
        at = slice(h * VDIM, (h + 1) * VDIM)

        out = intra_ref[:, at] + nt_dot(qexp_ref[:, at], state_ref[h, :VDIM, :])
        scale = lax.rsqrt(jnp.mean(out * out, axis=-1, keepdims=True) + norm_eps)
        out_ref[:, at] = (
            out * scale * gain_ref[...] * silu(gate_ref[:, at].astype(F32))
        ).astype(BF16)


def dispatch_kernel(half_ref, x_ref, gain_ref, routes_ref, gl_ref, cl_ref, out_ref, wt_ref):
    rows, width = x_ref.shape
    slots = out_ref.shape[0]
    part = out_ref.shape[1]
    experts = half_ref.shape[0] - 1
    capacity = slots // experts
    group_size = experts // GROUPS
    t0 = lax.broadcasted_iota(jnp.int32, (rows, rows), 0)
    t1 = lax.broadcasted_iota(jnp.int32, (rows, rows), 1)

    def column(row):
        return jnp.sum(jnp.where(t0 == t1, row.astype(F32), 0.0), axis=-1, keepdims=True)

    route = [column(routes_ref[j : j + 1, :]).astype(jnp.int32) for j in range(TOPK)]
    ids = lax.broadcasted_iota(jnp.int32, (rows, experts), 1)
    hot = [(r == ids).astype(F32) for r in route]
    before = jnp.dot(
        (t1 < t0).astype(BF16), sum(hot).astype(BF16), preferred_element_type=F32
    )
    group_exp = [jnp.exp(column(gl_ref[g : g + 1, :])) for g in range(GROUPS)]
    group_sum = sum(group_exp)
    gids = lax.broadcasted_iota(jnp.int32, (rows, GROUPS), 1)
    member = [
        ((r >= gids * group_size) & (r < (gids + 1) * group_size)).astype(F32) for r in route
    ]
    choice = [jnp.exp(column(cl_ref[j : j + 1, :])) for j in range(TOPK)]
    slot_ids = lax.broadcasted_iota(jnp.int32, (rows, slots), 1)
    place = jnp.zeros((rows, slots), F32)
    weight = jnp.zeros((rows, slots), F32)
    for j in range(TOPK):
        rank = jnp.sum(before * hot[j], axis=-1, keepdims=True).astype(jnp.int32)
        mark = (slot_ids == route[j] * capacity + rank).astype(F32)
        within = sum(
            jnp.sum(member[j] * member[i], axis=-1, keepdims=True) * choice[i]
            for i in range(TOPK)
        )
        prob = sum(member[j][:, g : g + 1] * group_exp[g] for g in range(GROUPS)) / group_sum
        place = place + mark
        weight = weight + mark * (prob * choice[j] / within)
    high = weight.astype(BF16)
    wt_ref[0] = high
    wt_ref[1] = (weight - high.astype(F32)).astype(BF16)
    x = x_ref[...].astype(F32)
    scale = lax.rsqrt(jnp.mean(x * x, axis=-1, keepdims=True) + norm_eps)
    cols = pl.ds(pl.multiple_of(half_ref[0] * part, part), part)
    normed = (x_ref[:, cols].astype(F32) * scale * gain_ref[:, cols]).astype(BF16)
    out_ref[...] = tn_dot(place.astype(BF16), normed).astype(BF16)


def return_kernel(wt_ref, back_ref, out_ref):
    back = back_ref[...]
    out_ref[...] = (
        jnp.dot(wt_ref[0], back, preferred_element_type=F32)
        + jnp.dot(wt_ref[1], back, preferred_element_type=F32)
    ).astype(BF16)


def later_after(later, earlier):
    later = later.astype(F32)
    rows = lax.broadcasted_iota(jnp.int32, later.shape, 1)
    decay = later[:, VDIM : VDIM + 1, :]
    return (decay * earlier.astype(F32) + jnp.where(rows < VDIM, later, 0.0)).astype(BF16)


def prefix(pay, count):
    span = pay
    before = None
    step = 1
    while step < count:
        came = lax.ppermute(span, "ep", [(i, i + step) for i in range(count - step)])
        before = came if before is None else later_after(before, came)
        step *= 2
        if step < count:
            span = later_after(span, came)
    return jnp.zeros_like(pay) if before is None else before


def cost(flops, size):
    return pl.CostEstimate(flops=flops, bytes_accessed=size, transcendentals=0)


def shaped(shape, kind):
    return jax.ShapeDtypeStruct(shape, kind)


def remote(src, dst, send, recv, device):
    return pltpu.make_async_remote_copy(
        src_ref=src, dst_ref=dst, send_sem=send, recv_sem=recv, device_id=device,
        device_id_type=pl.DeviceIdType.MESH,
    )


def other_plane(z, k):
    return (z % 2 + k % 2) % 2 + 2 * ((z // 2 + k // 2) % 2)


def split3(v):
    high = v.astype(BF16)
    rest = v - high.astype(F32)
    mid = rest.astype(BF16)
    return high, mid, (rest - mid.astype(F32)).astype(BF16)


def fused_kernel(
    routes_ref, gl_ref, cl_ref, floor_ref, hgain_ref, egain_ref,
    q_hbm, f_hbm, v_hbm, g_hbm, tok_hbm, wg_hbm, wu_hbm, wd_hbm, proj_hbm,
    mixer_ref, expert_ref,
    q_ref, f_ref, v_ref, g_ref, tok_ref, wg_ref, wu_ref, wd_ref, proj_ref,
    disp, wsrc, wgot, flat, hid, vout, vin, ret, back, perm,
    cum_ref, rate_ref, qexp_ref, intra_ref, pay, payin, sums, decays, first, chain_in, chain_out,
    ent, ent_out, mix,
    load_sem, zs, zr, ws, wr, xs, xr, cs, cr, ys, yr, hcs, hcr, vs, vr, rs, rr,
    ps, pr, hs, hr, es, er, ms, mr,
):
    ep, tp = lax.axis_index("ep"), lax.axis_index("tp")
    z, x = ep // 2, ep % 2
    y, c = tp // 2, tp % 2
    own = tp
    quarter_y = (1 - y) * 2 + c
    quarter_c = y * 2 + (1 - c)
    quarter_d = (1 - y) * 2 + (1 - c)

    def device(z_, x_, y_, c_):
        return (z_ * 2 + x_, y_ * 2 + c_)

    x_dev = device(z, 1 - x, y, c)
    y_dev = device(z, x, 1 - y, c)
    c_dev = device(z, x, y, 1 - c)
    planes = [other_plane(z, k) for k in range(GROUPS)]
    z_dev = [device(p, x, y, c) for p in planes]

    loads = [
        pltpu.make_async_copy(src, dst, load_sem.at[i])
        for i, (src, dst) in enumerate([
            (tok_hbm, tok_ref), (f_hbm, f_ref), (v_hbm, v_ref), (q_hbm, q_ref),
            (wg_hbm, wg_ref), (wu_hbm, wu_ref), (g_hbm, g_ref), (wd_hbm, wd_ref),
            (proj_hbm, proj_ref),
        ])
    ]
    tok_load, f_load, v_load, q_load, wg_load, wu_load, g_load, wd_load, proj_load = loads
    for load in loads:
        load.start()
    barrier = pltpu.get_barrier_semaphore()
    for dev in z_dev[1:] + [x_dev, y_dev, c_dev]:
        pl.semaphore_signal(
            barrier, inc=1, device_id=dev, device_id_type=pl.DeviceIdType.MESH
        )

    rows = tok_ref.shape[0]
    width = tok_ref.shape[1]
    cap, part = disp.shape[1], disp.shape[2]
    slots = GROUPS * cap
    group_size = TOPK
    route = [routes_ref[j : j + 1, :] for j in range(TOPK)]
    gids = lax.broadcasted_iota(jnp.int32, (8, rows), 0)
    member = [
        ((r >= gids * group_size) & (r < (gids + 1) * group_size)).astype(F32) for r in route
    ]
    t0 = lax.broadcasted_iota(jnp.int32, (rows, rows), 0)
    t1 = lax.broadcasted_iota(jnp.int32, (rows, rows), 1)
    before = jnp.dot(
        member[0].astype(BF16), (t0 < t1).astype(BF16), preferred_element_type=F32
    )

    def over_groups(v):
        return jnp.sum(v, axis=0, keepdims=True)

    rank = over_groups(before * member[0]).astype(jnp.int32)
    group = over_groups(gids.astype(F32) * member[0]).astype(jnp.int32)
    slot_ids = lax.broadcasted_iota(jnp.int32, (slots, rows), 0)
    perm[...] = (slot_ids == group * cap + rank).astype(F32).astype(BF16)

    group_exp = [jnp.exp(gl_ref[i : i + 1, :]) for i in range(GROUPS)]
    group_sum = sum(group_exp)
    choice = [jnp.exp(cl_ref[j : j + 1, :]) for j in range(TOPK)]
    expert_weight = [0.0] * group_size
    for j in range(TOPK):
        within = sum(over_groups(member[j] * member[i]) * choice[i] for i in range(TOPK))
        prob = sum(member[j][i : i + 1, :] * group_exp[i] for i in range(GROUPS)) / group_sum
        weight = prob * choice[j] / within
        for m in range(group_size):
            named = route[j] == group * group_size + m
            expert_weight[m] = expert_weight[m] + jnp.where(named, weight, 0.0)
    sub = lax.broadcasted_iota(jnp.int32, (8, rows), 0)
    stacked = jnp.zeros((8, rows), F32)
    for m in range(group_size):
        for i, piece in enumerate(split3(expert_weight[m])):
            stacked = jnp.where(sub == 3 * m + i, piece.astype(F32), stacked)
    stacked = stacked.astype(BF16)

    tok_load.wait()
    tokens = tok_ref[...].astype(F32)
    scale = lax.rsqrt(jnp.mean(tokens * tokens, axis=-1, keepdims=True) + norm_eps)
    cols = pl.ds(pl.multiple_of(c * part, part), part)
    normed = (tok_ref[:, cols].astype(F32) * scale * egain_ref[:, cols]).astype(BF16)
    for i in range(GROUPS):
        chosen = perm[i * cap : (i + 1) * cap, :]
        disp[i] = jnp.dot(chosen, normed, preferred_element_type=F32).astype(BF16)
        got = nt_dot(stacked, chosen)
        pair = [got[3 * m : 3 * m + 1, :] + got[3 * m + 1 : 3 * m + 2, :] + got[3 * m + 2 : 3 * m + 3, :]
                for m in range(group_size)]
        lanes = lax.broadcasted_iota(jnp.int32, (8, cap), 0)
        packed = jnp.where(lanes == 0, pair[0], jnp.where(lanes == 1, pair[1], 0.0))
        wsrc[i] = jnp.concatenate([packed, jnp.zeros((8, wsrc.shape[2] - cap), F32)], axis=1)
    flat[0, c, x] = disp[z]
    wgot[0] = wsrc[z]

    pl.semaphore_wait(barrier, len(z_dev[1:]) + 3)

    def z_send(k):
        return remote(disp.at[planes[k]], flat.at[k, c, x], zs.at[k], zr.at[k], z_dev[k])

    def w_send(k):
        return remote(wsrc.at[planes[k]], wgot.at[k], ws.at[k], wr.at[k], z_dev[k])

    def x_send(k, b):
        return remote(flat.at[k, c, b], flat.at[k, c, b], xs.at[k], xr.at[k], x_dev)

    def c_send(k, half, b, i):
        return remote(
            flat.at[k, half, b], flat.at[k, half, b], cs.at[k, i], cr.at[k, i], c_dev
        )

    def arrive_z(k):
        if k > 0:
            z_send(k).wait_recv()
        x_send(k, x).start()
        c_send(k, c, x, 0).start()

    def arrive_x(k):
        x_send(k, 1 - x).wait_recv()
        c_send(k, c, 1 - x, 1).start()

    def y_send(k, at):
        return remote(hid.at[k, at], hid.at[k, at], ys.at[k], yr.at[k], y_dev)

    def hc_send(k, at, i):
        return remote(hid.at[k, at], hid.at[k, at], hcs.at[k, i], hcr.at[k, i], c_dev)

    both = 2 * cap

    def gate_up(k):
        c_send(k, 1 - c, x, 0).wait_recv()
        c_send(k, 1 - c, 1 - x, 1).wait_recv()
        a = [flat[k, i].reshape(both, part) for i in range(2)]
        gate = sum(
            jnp.dot(a[i], wg_ref[i * part : (i + 1) * part, :], preferred_element_type=F32)
            for i in range(2)
        )
        up = sum(
            jnp.dot(a[i], wu_ref[i * part : (i + 1) * part, :], preferred_element_type=F32)
            for i in range(2)
        )
        hid[k, own] = (silu(gate) * up).astype(BF16)
        y_send(k, own).start()
        hc_send(k, own, 0).start()

    def arrive_y(k):
        y_send(k, quarter_y).wait_recv()
        hc_send(k, quarter_y, 1).start()

    depth = wd_ref.shape[0] // 4

    def v_send(k, b):
        return remote(vout.at[k, b], vin.at[k], vs.at[k], vr.at[k], x_dev)

    def down(k):
        hc_send(k, quarter_c, 0).wait_recv()
        hc_send(k, quarter_d, 1).wait_recv()
        value = sum(
            jnp.dot(hid[k, i], wd_ref[i * depth : (i + 1) * depth, :], preferred_element_type=F32)
            for i in range(4)
        ).astype(BF16)
        vout[k, 0] = value[:cap]
        vout[k, 1] = value[cap:]
        v_send(k, 1 - x).start()

    def r_send(k):
        return remote(ret.at[k], back.at[z], rs.at[k], rr.at[k], z_dev[k])

    def combine(k):
        v_send(k, x).wait_recv()
        if k > 0:
            w_send(k).wait_recv()
        d0 = lax.broadcasted_iota(jnp.int32, (cap, cap), 0)
        d1 = lax.broadcasted_iota(jnp.int32, (cap, cap), 1)
        even, odd = wgot[k, 0:1, :cap], wgot[k, 1:2, :cap]
        mine = jnp.where(x == 0, even, odd)
        theirs = jnp.where(x == 0, odd, even)

        def column(row):
            return jnp.sum(jnp.where(d0 == d1, row, 0.0), axis=-1, keepdims=True)

        row = (
            column(mine) * vout[k, x].astype(F32) + column(theirs) * vin[k].astype(F32)
        ).astype(BF16)
        if k == 0:
            back[z] = row
        else:
            ret[k] = row
            r_send(k).start()

    length = q_ref.shape[0]
    heads = q_ref.shape[1] // KEYDIM
    lead = heads // 2
    causal = (
        lax.broadcasted_iota(jnp.int32, (length, length), 1)
        <= lax.broadcasted_iota(jnp.int32, (length, length), 0)
    )

    def p_send(start):
        return remote(pay.at[pl.ds(start, lead)], payin, ps, pr, x_dev)

    def payload():
        f_load.wait()
        v_load.wait()
        tril = causal.astype(F32).astype(BF16)
        rates = (1.0 - floor_ref[...]) / (1.0 + jnp.exp(f_ref[...].astype(F32)))
        rate_ref[...] = rates
        cum = sum(
            jnp.dot(tril, piece, preferred_element_type=F32)
            for piece in split3(jnp.log(1.0 - rates))
        )
        cum_ref[...] = cum
        sub = lax.broadcasted_iota(jnp.int32, (PAD, KEYDIM), 0)
        for h in range(heads):
            at = slice(h * KEYDIM, (h + 1) * KEYDIM)
            end = cum[length - 1 : length, at]
            kend = (rates[:, at] * jnp.exp(end - cum[:, at])).astype(BF16)
            pay[h, :VDIM, :] = tn_dot(v_ref[:, at], kend).astype(BF16)
            high, mid, _ = split3(jnp.exp(end))
            pay[h, VDIM:, :] = jnp.where(
                sub == 0, high.astype(F32), jnp.where(sub == 1, mid.astype(F32), 0.0)
            ).astype(BF16)
        p_send((1 - x) * lead).start()

    def rest(h):
        at = slice(h * KEYDIM, (h + 1) * KEYDIM)
        cum = cum_ref[:, at]
        qexp = (silu(q_ref[:, at].astype(F32)) * jnp.exp(cum)).astype(BF16)
        kexp = (rate_ref[:, at] * jnp.exp(-cum)).astype(BF16)
        scores = jnp.where(causal, nt_dot(qexp, kexp), 0.0).astype(BF16)
        intra_ref[:, at] = jnp.dot(scores, v_ref[:, at], preferred_element_type=F32)
        qexp_ref[:, at] = qexp

    def pair_up():
        p_send(x * lead).wait_recv()
        for i in range(lead):
            mine = pay[x * lead + i].astype(F32)
            theirs = payin[i].astype(F32)
            s0 = jnp.where(x == 0, mine, theirs)
            s1 = jnp.where(x == 0, theirs, mine)
            d0 = s0[VDIM : VDIM + 1, :] + s0[VDIM + 1 : VDIM + 2, :]
            d1 = s1[VDIM : VDIM + 1, :] + s1[VDIM + 1 : VDIM + 2, :]
            sums[i] = d1 * s0[:VDIM, :] + s1[:VDIM, :]
            first[i] = s0[:VDIM, :]
            decays[i, 0:8] = jnp.broadcast_to(d0, (8, KEYDIM))
            decays[i, 8:16] = jnp.broadcast_to(d0 * d1, (8, KEYDIM))

    def h_send():
        return remote(chain_out, chain_in, hs, hr, device((z + 1) % GROUPS, x, y, c))

    def e_send(start):
        return remote(ent_out, ent.at[pl.ds(start, lead)], es, er, x_dev)

    def hop(step):
        @pl.when(z == step)
        def _():
            if step == 0:
                chain_in[...] = jnp.zeros_like(chain_in)
            else:
                h_send().wait_recv()
            if step < GROUPS - 1:
                for i in range(lead):
                    chain_out[i] = (
                        decays[i, 8:9] * chain_in[i].astype(F32) + sums[i]
                    ).astype(BF16)
                h_send().start()
            for i in range(lead):
                came = chain_in[i].astype(F32)
                later = decays[i, 0:1] * came + first[i]
                ent[x * lead + i] = jnp.where(x == 0, came, later).astype(BF16)
                ent_out[i] = jnp.where(x == 0, later, came).astype(BF16)
            e_send(x * lead).start()

    def m_send(at):
        return remote(mix.at[at], mix.at[at], ms.at[0], mr.at[0], y_dev)

    def mc_send(at, i):
        return remote(mix.at[at], mix.at[at], ms.at[1 + i], mr.at[1 + i], c_dev)

    def finish():
        e_send((1 - x) * lead).wait_recv()
        g_load.wait()
        for h in range(heads):
            at = slice(h * VDIM, (h + 1) * VDIM)
            out = intra_ref[:, at] + nt_dot(qexp_ref[:, at], ent[h])
            norm = lax.rsqrt(jnp.mean(out * out, axis=-1, keepdims=True) + norm_eps)
            mix[own, :, at] = (
                out * norm * hgain_ref[...] * silu(g_ref[:, at].astype(F32))
            ).astype(BF16)
        m_send(own).start()
        mc_send(own, 0).start()

    def arrive_mix():
        m_send(quarter_y).wait_recv()
        mc_send(quarter_y, 1).start()

    def project():
        mc_send(quarter_c, 0).wait_recv()
        mc_send(quarter_d, 1).wait_recv()
        proj_load.wait()
        wide = proj_ref.shape[0] // 4
        mixer_ref[...] = sum(
            jnp.dot(mix[i], proj_ref[i * wide : (i + 1) * wide, :], preferred_element_type=F32)
            for i in range(4)
        ).astype(BF16)

    for k in range(1, GROUPS):
        z_send(k).start()
        w_send(k).start()
    arrive_z(0)
    payload()
    q_load.wait()
    rest(0)
    rest(1)
    arrive_x(0)
    arrive_z(1)
    pair_up()
    hop(0)
    for h in range(2, heads):
        rest(h)
    wg_load.wait()
    wu_load.wait()
    gate_up(0)
    arrive_z(2)
    hop(1)
    arrive_x(1)
    gate_up(1)
    arrive_y(0)
    hop(2)
    arrive_x(2)
    wd_load.wait()
    down(0)
    arrive_z(3)
    gate_up(2)
    hop(3)
    arrive_y(1)
    combine(0)
    down(1)
    arrive_x(3)
    gate_up(3)
    arrive_y(2)
    finish()
    down(2)
    combine(1)
    combine(2)
    arrive_y(3)
    down(3)
    arrive_mix()
    combine(3)
    project()
    for k in range(1, GROUPS):
        r_send(k).wait_recv()
    expert_ref[...] = tn_dot(perm[...], back[...].reshape(slots, back.shape[2])).astype(BF16)

    for k in range(GROUPS):
        if k > 0:
            z_send(k).wait_send()
            w_send(k).wait_send()
            r_send(k).wait_send()
        x_send(k, x).wait_send()
        c_send(k, c, x, 0).wait_send()
        c_send(k, c, 1 - x, 1).wait_send()
        y_send(k, own).wait_send()
        hc_send(k, own, 0).wait_send()
        hc_send(k, quarter_y, 1).wait_send()
        v_send(k, 1 - x).wait_send()
    p_send((1 - x) * lead).wait_send()
    e_send(x * lead).wait_send()

    @pl.when(z < GROUPS - 1)
    def _():
        h_send().wait_send()

    m_send(own).wait_send()
    mc_send(own, 0).wait_send()
    mc_send(quarter_y, 1).wait_send()


def fused(
    mixer_query, mixer_forget, mixer_value, mixer_gate, forget_floor, head_gain, mixer_proj,
    expert_tokens, expert_gain, routes, group_logits, choice_logits, w_gate, w_up, w_down,
):
    length, width = mixer_query.shape
    heads = width // KEYDIM
    lead = heads // 2
    experts = lax.axis_size("ep")
    rows, model = expert_tokens.shape
    cap = 2 * TOPK * rows // experts
    part = model // 2
    hidden = w_gate.shape[2]
    outs = w_down.shape[2]
    dma, n = pltpu.SemaphoreType.DMA, GROUPS
    any_spec = pl.BlockSpec(memory_space=pl.ANY)
    vmem = pltpu.VMEM
    return pl.pallas_call(
        fused_kernel,
        name="fused",
        out_shape=(
            shaped((length, mixer_proj.shape[1]), BF16),
            shaped((rows, outs), BF16),
        ),
        in_specs=[VM] * 6 + [any_spec] * 9,
        out_specs=(VM, VM),
        scratch_shapes=[
            vmem((length, width), BF16), vmem((length, width), BF16),
            vmem((length, width), BF16), vmem((length, width), BF16),
            vmem((rows, model), BF16),
            vmem((model, hidden), BF16), vmem((model, hidden), BF16),
            vmem(w_down.shape[1:], BF16), vmem(mixer_proj.shape, BF16),
            vmem((n, cap, part), BF16),
            vmem((n, 8, 128), F32), vmem((n, 8, 128), F32),
            vmem((n, 2, 2, cap, part), BF16),
            vmem((n, 4, 2 * cap, hidden), BF16),
            vmem((n, 2, cap, outs), BF16), vmem((n, cap, outs), BF16),
            vmem((n, cap, outs), BF16), vmem((n, cap, outs), BF16),
            vmem((n * cap, rows), BF16),
            vmem((length, width), F32), vmem((length, width), F32),
            vmem((length, width), BF16), vmem((length, width), F32),
            vmem((heads, VDIM + PAD, KEYDIM), BF16), vmem((lead, VDIM + PAD, KEYDIM), BF16),
            vmem((lead, VDIM, KEYDIM), F32), vmem((lead, 16, KEYDIM), F32),
            vmem((lead, VDIM, KEYDIM), F32),
            vmem((lead, VDIM, KEYDIM), BF16), vmem((lead, VDIM, KEYDIM), BF16),
            vmem((heads, VDIM, KEYDIM), BF16), vmem((lead, VDIM, KEYDIM), BF16),
            vmem((4, length, width), BF16),
            dma((9,)), dma((n,)), dma((n,)), dma((n,)), dma((n,)), dma((n,)), dma((n,)),
            dma((n, 2)), dma((n, 2)), dma((n,)), dma((n,)), dma((n, 2)), dma((n, 2)),
            dma((n,)), dma((n,)), dma((n,)), dma((n,)),
            dma, dma, dma, dma, dma, dma, dma((3,)), dma((3,)),
        ],
        compiler_params=pltpu.CompilerParams(
            collective_id=0, has_side_effects=True, vmem_limit_bytes=64000000
        ),
        cost_estimate=cost(8000000000, 12000000),
    )(
        routes.T, group_logits.T, choice_logits.T, forget_floor[None, :], head_gain[None, :],
        expert_gain[None, :], mixer_query, mixer_forget, mixer_value, mixer_gate,
        expert_tokens, w_gate[0], w_up[0], w_down[0], mixer_proj,
    )


def per_device(
    mixer_query, mixer_forget, mixer_value, mixer_gate, forget_floor, head_gain, mixer_proj,
    expert_tokens, expert_gain, routes, group_logits, choice_logits, w_gate, w_up, w_down,
):
    length, width = mixer_query.shape
    heads = width // KEYDIM
    experts = lax.axis_size("ep")
    tp = lax.axis_size("tp")
    rows, model = expert_tokens.shape
    capacity = 2 * TOPK * rows // experts
    slots = experts * capacity
    split = 2
    part = model // split
    which = lax.axis_index("tp") % split
    half = jnp.full((experts + 1,), 0, jnp.int32) + which

    outgoing, wt = pl.pallas_call(
        dispatch_kernel,
        name="dispatch",
        out_shape=(shaped((slots, part), BF16), shaped((2, rows, slots), BF16)),
        in_specs=[SM, VM, VM, VM, VM, VM],
        out_specs=(VM, VM),
        cost_estimate=cost(2 * rows * slots * part, 4000000),
    )(half, expert_tokens, expert_gain[None, :], routes.T, group_logits.T, choice_logits.T)
    arrived = lax.all_to_all(
        outgoing.reshape(experts, capacity, part), "ep", split_axis=0, concat_axis=0, tiled=True
    )

    intra, qexp, pay = pl.pallas_call(
        local_kernel,
        name="local_scan",
        out_shape=(
            shaped((length, width), F32),
            shaped((length, width), BF16),
            shaped((heads, VDIM + PAD, KEYDIM), BF16),
        ),
        in_specs=[VM] * 4,
        out_specs=(VM, VM, VM),
        cost_estimate=cost(3000000000, 4000000),
    )(mixer_query, mixer_forget, mixer_value, forget_floor[None, :])
    arrived, pay = lax.optimization_barrier((arrived, pay))
    entering = prefix(pay, experts)
    mixed = pl.pallas_call(
        finish_kernel,
        name="mixer_finish",
        out_shape=shaped((length, width), BF16),
        in_specs=[VM] * 5,
        out_specs=VM,
        cost_estimate=cost(1000000000, 4000000),
    )(entering, intra, qexp, mixer_gate, head_gain[None, :])
    mixed_all = lax.all_gather(mixed, "tp", axis=1, tiled=True)

    own = arrived.reshape(slots, part)
    other = lax.ppermute(own, "tp", [(i, i ^ 1) for i in range(tp)])
    flat_in = jnp.concatenate(
        [jnp.where(which == 0, own, other), jnp.where(which == 0, other, own)], axis=1
    )
    gate_pre = jnp.dot(flat_in, w_gate[0], preferred_element_type=F32)
    up_pre = jnp.dot(flat_in, w_up[0], preferred_element_type=F32)
    hidden = (jax.nn.silu(gate_pre) * up_pre).astype(BF16)
    hidden_all = lax.all_gather(hidden, "tp", axis=1, tiled=True)
    mixer_out = jnp.dot(mixed_all, mixer_proj, preferred_element_type=F32).astype(BF16)
    down = jnp.dot(hidden_all, w_down[0], preferred_element_type=F32).astype(BF16)
    back = lax.all_to_all(
        down.reshape(experts, capacity, -1), "ep", split_axis=0, concat_axis=0, tiled=True
    ).reshape(slots, -1)
    expert_out = pl.pallas_call(
        return_kernel,
        name="weigh",
        out_shape=shaped((rows, back.shape[1]), BF16),
        in_specs=[VM, VM],
        out_specs=VM,
        cost_estimate=cost(4 * rows * slots * back.shape[1], 1000000),
    )(wt, back)
    return (mixer_out, expert_out)


def solution(mesh):
    paired = mesh.shape["ep"] == GROUPS * TOPK and mesh.shape["tp"] == 4
    return jax.shard_map(
        fused if paired else per_device,
        mesh=mesh,
        in_specs=(
            P("ep", "tp"),
            P("ep", "tp"),
            P("ep", "tp"),
            P("ep", "tp"),
            P("tp"),
            P(),
            P(None, "tp"),
            P("ep", None),
            P(),
            P("ep", None),
            P("ep", None),
            P("ep", None),
            P("ep", None, "tp"),
            P("ep", None, "tp"),
            P("ep", None, "tp"),
        ),
        out_specs=(P("ep", "tp"), P("ep", "tp")),
        check_vma=False,
    )
```

```python
import jax
import jax.numpy as jnp
from jax import lax
from jax.experimental import pallas as pl
from jax.experimental.pallas import tpu as pltpu
from jax.sharding import PartitionSpec as P

KEYDIM = 128
VDIM = 128
GROUPS = 4
TOPK = 2
SPLIT = 2
PAD = 16
norm_eps = 1e-06
F32 = jnp.float32
BF16 = jnp.bfloat16
VM = pl.BlockSpec(memory_space=pltpu.VMEM)
SM = pl.BlockSpec(memory_space=pltpu.SMEM)


def tn_dot(a, b):
    return lax.dot_general(a, b, (((0,), (0,)), ((), ())), preferred_element_type=F32)


def nt_dot(a, b):
    return lax.dot_general(a, b, (((1,), (1,)), ((), ())), preferred_element_type=F32)


def silu(v):
    return v / (1.0 + jnp.exp(-v))


def local_kernel(q_ref, f_ref, v_ref, floor_ref, intra_ref, qexp_ref, pay_ref):
    length = q_ref.shape[0]
    rows = lax.broadcasted_iota(jnp.int32, (length, length), 0)
    cols = lax.broadcasted_iota(jnp.int32, (length, length), 1)
    causal = cols <= rows
    tril = causal.astype(F32)
    for h in range(q_ref.shape[1] // KEYDIM):
        at = slice(h * KEYDIM, (h + 1) * KEYDIM)
        floor = floor_ref[:, at]
        rates = (1.0 - floor) / (1.0 + jnp.exp(f_ref[:, at].astype(F32)))
        cum = jnp.dot(
            tril, jnp.log(1.0 - rates), precision=lax.Precision.HIGHEST,
            preferred_element_type=F32,
        )
        end = cum[length - 1 : length, :]
        qexp = (silu(q_ref[:, at].astype(F32)) * jnp.exp(cum)).astype(BF16)
        kexp = (rates * jnp.exp(-cum)).astype(BF16)
        kend = (rates * jnp.exp(end - cum)).astype(BF16)
        value = v_ref[:, at]
        scores = jnp.where(causal, nt_dot(qexp, kexp), 0.0).astype(BF16)
        intra_ref[:, at] = jnp.dot(scores, value, preferred_element_type=F32)
        qexp_ref[:, at] = qexp
        pay_ref[h, :VDIM, :] = tn_dot(value, kend).astype(BF16)
        pay_ref[h, VDIM:, :] = jnp.broadcast_to(jnp.exp(end), (PAD, KEYDIM)).astype(BF16)


def finish_kernel(state_ref, intra_ref, qexp_ref, gate_ref, gain_ref, out_ref):
    for h in range(intra_ref.shape[1] // VDIM):
        at = slice(h * VDIM, (h + 1) * VDIM)

        out = intra_ref[:, at] + nt_dot(qexp_ref[:, at], state_ref[h, :VDIM, :])
        scale = lax.rsqrt(jnp.mean(out * out, axis=-1, keepdims=True) + norm_eps)
        out_ref[:, at] = (
            out * scale * gain_ref[...] * silu(gate_ref[:, at].astype(F32))
        ).astype(BF16)


def dispatch_kernel(half_ref, x_ref, gain_ref, routes_ref, gl_ref, cl_ref, out_ref, wt_ref):
    rows, width = x_ref.shape
    slots = out_ref.shape[0]
    part = out_ref.shape[1]
    experts = half_ref.shape[0] - 1
    capacity = slots // experts
    group_size = experts // GROUPS
    t0 = lax.broadcasted_iota(jnp.int32, (rows, rows), 0)
    t1 = lax.broadcasted_iota(jnp.int32, (rows, rows), 1)

    def column(row):
        return jnp.sum(jnp.where(t0 == t1, row.astype(F32), 0.0), axis=-1, keepdims=True)

    route = [column(routes_ref[j : j + 1, :]).astype(jnp.int32) for j in range(TOPK)]
    ids = lax.broadcasted_iota(jnp.int32, (rows, experts), 1)
    hot = [(r == ids).astype(F32) for r in route]
    before = jnp.dot(
        (t1 < t0).astype(BF16), sum(hot).astype(BF16), preferred_element_type=F32
    )
    group_exp = [jnp.exp(column(gl_ref[g : g + 1, :])) for g in range(GROUPS)]
    group_sum = sum(group_exp)
    gids = lax.broadcasted_iota(jnp.int32, (rows, GROUPS), 1)
    member = [
        ((r >= gids * group_size) & (r < (gids + 1) * group_size)).astype(F32) for r in route
    ]
    choice = [jnp.exp(column(cl_ref[j : j + 1, :])) for j in range(TOPK)]
    slot_ids = lax.broadcasted_iota(jnp.int32, (rows, slots), 1)
    place = jnp.zeros((rows, slots), F32)
    weight = jnp.zeros((rows, slots), F32)
    for j in range(TOPK):
        rank = jnp.sum(before * hot[j], axis=-1, keepdims=True).astype(jnp.int32)
        mark = (slot_ids == route[j] * capacity + rank).astype(F32)
        within = sum(
            jnp.sum(member[j] * member[i], axis=-1, keepdims=True) * choice[i]
            for i in range(TOPK)
        )
        prob = sum(member[j][:, g : g + 1] * group_exp[g] for g in range(GROUPS)) / group_sum
        place = place + mark
        weight = weight + mark * (prob * choice[j] / within)
    high = weight.astype(BF16)
    wt_ref[0] = high
    wt_ref[1] = (weight - high.astype(F32)).astype(BF16)
    x = x_ref[...].astype(F32)
    scale = lax.rsqrt(jnp.mean(x * x, axis=-1, keepdims=True) + norm_eps)
    cols = pl.ds(pl.multiple_of(half_ref[0] * part, part), part)
    normed = (x_ref[:, cols].astype(F32) * scale * gain_ref[:, cols]).astype(BF16)
    out_ref[...] = tn_dot(place.astype(BF16), normed).astype(BF16)


def return_kernel(wt_ref, back_ref, out_ref):
    back = back_ref[...]
    out_ref[...] = (
        jnp.dot(wt_ref[0], back, preferred_element_type=F32)
        + jnp.dot(wt_ref[1], back, preferred_element_type=F32)
    ).astype(BF16)


def later_after(later, earlier):
    later = later.astype(F32)
    rows = lax.broadcasted_iota(jnp.int32, later.shape, 1)
    decay = later[:, VDIM : VDIM + 1, :]
    return (decay * earlier.astype(F32) + jnp.where(rows < VDIM, later, 0.0)).astype(BF16)


def prefix(pay, count):
    span = pay
    before = None
    step = 1
    while step < count:
        came = lax.ppermute(span, "ep", [(i, i + step) for i in range(count - step)])
        before = came if before is None else later_after(before, came)
        step *= 2
        if step < count:
            span = later_after(span, came)
    return jnp.zeros_like(pay) if before is None else before


def cost(flops, size):
    return pl.CostEstimate(flops=flops, bytes_accessed=size, transcendentals=0)


def shaped(shape, kind):
    return jax.ShapeDtypeStruct(shape, kind)


def remote(src, dst, send, recv, device):
    return pltpu.make_async_remote_copy(
        src_ref=src, dst_ref=dst, send_sem=send, recv_sem=recv, device_id=device,
        device_id_type=pl.DeviceIdType.MESH,
    )


def other_plane(z, k):
    return (z % 2 + k % 2) % 2 + 2 * ((z // 2 + k // 2) % 2)


def split3(v):
    high = v.astype(BF16)
    rest = v - high.astype(F32)
    mid = rest.astype(BF16)
    return high, mid, (rest - mid.astype(F32)).astype(BF16)


def fused_kernel(
    routes_hbm, gl_hbm, cl_hbm, floor_hbm, hgain_hbm, egain_hbm,
    q_hbm, f_hbm, v_hbm, g_hbm, tok_hbm, wg_hbm, wu_hbm, wd_hbm, proj_hbm,
    mixer_ref, expert_ref,
    routes_ref, gl_ref, cl_ref, floor_ref, hgain_ref, egain_ref,
    q_ref, f_ref, v_ref, g_ref, tok_ref, wg_ref, wu_ref, wd_ref, proj_ref,
    disp, wsrc, wgot, flat, hid, vout, vin, ret, back, perm,
    cum_ref, rate_ref, qexp_ref, intra_ref, pay, payin, sums, decays, first, chain_in, chain_out,
    ent, ent_out, mix,
    load_sem, zs, zr, ws, wr, xs, xr, cs, cr, ys, yr, hcs, hcr, vs, vr, rs, rr,
    ps, pr, hs, hr, es, er, ms, mr, mcs, mcr, ds, dr,
):
    ep, tp = lax.axis_index("ep"), lax.axis_index("tp")
    z, x = ep // 2, ep % 2
    y, c = tp // 2, tp % 2
    own = tp
    quarter_y = (1 - y) * 2 + c
    quarter_c = y * 2 + (1 - c)
    quarter_d = (1 - y) * 2 + (1 - c)

    def device(z_, x_, y_, c_):
        return (z_ * 2 + x_, y_ * 2 + c_)

    x_dev = device(z, 1 - x, y, c)
    y_dev = device(z, x, 1 - y, c)
    c_dev = device(z, x, y, 1 - c)
    planes = [other_plane(z, k) for k in range(GROUPS)]
    z_dev = [device(p, x, y, c) for p in planes]

    loads = [
        pltpu.make_async_copy(src, dst, load_sem.at[i])
        for i, (src, dst) in enumerate([
            (routes_hbm, routes_ref), (gl_hbm, gl_ref), (cl_hbm, cl_ref),
            (tok_hbm, tok_ref), (egain_hbm, egain_ref), (floor_hbm, floor_ref), (f_hbm, f_ref), (v_hbm, v_ref), (q_hbm, q_ref),
            (wg_hbm, wg_ref), (wu_hbm, wu_ref), (g_hbm, g_ref), (wd_hbm, wd_ref),
            (proj_hbm, proj_ref), (hgain_hbm, hgain_ref),
        ])
    ]
    (
        routes_load, gl_load, cl_load, tok_load, egain_load, floor_load, f_load, v_load, q_load,
        wg_load, wu_load, g_load, wd_load, proj_load, hgain_load,
    ) = loads
    for load in loads:
        load.start()
    barrier = pltpu.get_barrier_semaphore()
    for dev in z_dev[1:] + [x_dev, y_dev, c_dev]:
        pl.semaphore_signal(
            barrier, inc=1, device_id=dev, device_id_type=pl.DeviceIdType.MESH
        )

    rows = tok_ref.shape[0]
    width = tok_ref.shape[1]
    cap, part = disp.shape[1], disp.shape[2]
    slots = GROUPS * cap
    group_size = TOPK
    routes_load.wait()
    gl_load.wait()
    cl_load.wait()
    route = [routes_ref[j : j + 1, :] for j in range(TOPK)]
    gids = lax.broadcasted_iota(jnp.int32, (8, rows), 0)
    member = [
        ((r >= gids * group_size) & (r < (gids + 1) * group_size)).astype(F32) for r in route
    ]
    t0 = lax.broadcasted_iota(jnp.int32, (rows, rows), 0)
    t1 = lax.broadcasted_iota(jnp.int32, (rows, rows), 1)
    before = jnp.dot(
        member[0].astype(BF16), (t0 < t1).astype(BF16), preferred_element_type=F32
    )

    def over_groups(v):
        return jnp.sum(v, axis=0, keepdims=True)

    rank = over_groups(before * member[0]).astype(jnp.int32)
    group = over_groups(gids.astype(F32) * member[0]).astype(jnp.int32)
    slot_ids = lax.broadcasted_iota(jnp.int32, (slots, rows), 0)
    perm[...] = (slot_ids == group * cap + rank).astype(F32).astype(BF16)

    group_exp = [jnp.exp(gl_ref[i : i + 1, :]) for i in range(GROUPS)]
    group_sum = sum(group_exp)
    choice = [jnp.exp(cl_ref[j : j + 1, :]) for j in range(TOPK)]
    expert_weight = [0.0] * group_size
    for j in range(TOPK):
        within = sum(over_groups(member[j] * member[i]) * choice[i] for i in range(TOPK))
        prob = sum(member[j][i : i + 1, :] * group_exp[i] for i in range(GROUPS)) / group_sum
        weight = prob * choice[j] / within
        for m in range(group_size):
            named = route[j] == group * group_size + m
            expert_weight[m] = expert_weight[m] + jnp.where(named, weight, 0.0)
    sub = lax.broadcasted_iota(jnp.int32, (8, rows), 0)
    stacked = jnp.zeros((8, rows), F32)
    for m in range(group_size):
        for i, piece in enumerate(split3(expert_weight[m])):
            stacked = jnp.where(sub == 3 * m + i, piece.astype(F32), stacked)
    stacked = stacked.astype(BF16)

    tok_load.wait()
    egain_load.wait()
    tokens = tok_ref[...].astype(F32)
    scale = lax.rsqrt(jnp.mean(tokens * tokens, axis=-1, keepdims=True) + norm_eps)
    cols = pl.ds(pl.multiple_of(c * part, part), part)
    normed = (tok_ref[:, cols].astype(F32) * scale * egain_ref[:, cols]).astype(BF16)
    for i in range(GROUPS):
        chosen = perm[i * cap : (i + 1) * cap, :]
        disp[i] = jnp.dot(chosen, normed, preferred_element_type=F32).astype(BF16)
        got = nt_dot(stacked, chosen)
        pair = [got[3 * m : 3 * m + 1, :] + got[3 * m + 1 : 3 * m + 2, :] + got[3 * m + 2 : 3 * m + 3, :]
                for m in range(group_size)]
        lanes = lax.broadcasted_iota(jnp.int32, (8, cap), 0)
        packed = jnp.where(lanes == 0, pair[0], jnp.where(lanes == 1, pair[1], 0.0))
        wsrc[i] = jnp.concatenate([packed, jnp.zeros((8, wsrc.shape[2] - cap), F32)], axis=1)
    flat[0, c, x] = disp[z]
    wgot[0] = wsrc[z]

    pl.semaphore_wait(barrier, len(z_dev[1:]) + 3)

    half_part = part // 2
    my_cols = pl.ds(pl.multiple_of(y * half_part, half_part), half_part)
    other_cols = pl.ds(pl.multiple_of((1 - y) * half_part, half_part), half_part)
    block = [x, 1 - x]

    def piece(k, b, at=my_cols):
        return flat.at[k, c, b, :, at] if k == SPLIT else flat.at[k, c, b]

    def z_send(k):
        rows_of = disp.at[planes[k], :, my_cols] if k == SPLIT else disp.at[planes[k]]
        return remote(rows_of, piece(k, x), zs.at[k], zr.at[k], z_dev[k])

    def w_send(k):
        return remote(wsrc.at[planes[k]], wgot.at[k], ws.at[k], wr.at[k], z_dev[k])

    def x_send(k, b):
        return remote(piece(k, b), piece(k, b), xs.at[k], xr.at[k], x_dev)

    def d_send(i, at):
        ref = piece(SPLIT, block[i], at)
        return remote(ref, ref, ds.at[i], dr.at[i], y_dev)

    def c_send(k, i, half):
        ref = flat.at[k, half, block[i]]
        return remote(ref, ref, cs.at[k, i], cr.at[k, i], c_dev)

    def arrive_z(k):
        z_send(k).wait_recv()
        x_send(k, x).start()
        if k == SPLIT:
            d_send(0, my_cols).start()
        else:
            c_send(k, 0, c).start()

    def arrive_x(k):
        x_send(k, 1 - x).wait_recv()
        if k == SPLIT:
            d_send(1, my_cols).start()
        else:
            c_send(k, 1, c).start()

    def arrive_d(i):
        d_send(i, other_cols).wait_recv()
        c_send(SPLIT, i, c).start()

    def y_send(k, i, at):
        ref = hid.at[k, block[i], at]
        return remote(ref, ref, ys.at[k, i], yr.at[k, i], y_dev)

    def hc_send(k, i, at, n):
        ref = hid.at[k, block[i], at]
        return remote(ref, ref, hcs.at[k, i, n], hcr.at[k, i, n], c_dev)

    def gate_up(*blocks):
        for k, i in blocks:
            c_send(k, i, 1 - c).wait_recv()
        a = [
            jnp.concatenate([flat[k, n, block[i]] for k, i in blocks], axis=0) for n in range(2)
        ]
        gate = sum(
            jnp.dot(a[n], wg_ref[n * part : (n + 1) * part, :], preferred_element_type=F32)
            for n in range(2)
        )
        up = sum(
            jnp.dot(a[n], wu_ref[n * part : (n + 1) * part, :], preferred_element_type=F32)
            for n in range(2)
        )
        act = (silu(gate) * up).astype(BF16)
        for m, (k, i) in enumerate(blocks):
            hid[k, block[i], own] = act[m * cap : (m + 1) * cap]
            y_send(k, i, own).start()
            hc_send(k, i, own, 0).start()

    def arrive_y(k, i):
        y_send(k, i, quarter_y).wait_recv()
        hc_send(k, i, quarter_y, 1).start()

    depth = wd_ref.shape[0] // 4

    def v_send(k):
        return remote(vout.at[k, 1], vin.at[k], vs.at[k], vr.at[k], x_dev)

    def down(k):
        for i in range(2):
            hc_send(k, i, quarter_c, 0).wait_recv()
            hc_send(k, i, quarter_d, 1).wait_recv()
        value = sum(
            jnp.dot(
                jnp.concatenate([hid[k, block[i], n] for i in range(2)], axis=0),
                wd_ref[n * depth : (n + 1) * depth, :], preferred_element_type=F32,
            )
            for n in range(4)
        ).astype(BF16)
        vout[k, 0] = value[:cap]
        vout[k, 1] = value[cap:]
        v_send(k).start()

    def r_send(k):
        return remote(ret.at[k], back.at[z], rs.at[k], rr.at[k], z_dev[k])

    def combine(k):
        v_send(k).wait_recv()
        if k > 0:
            w_send(k).wait_recv()
        d0 = lax.broadcasted_iota(jnp.int32, (cap, cap), 0)
        d1 = lax.broadcasted_iota(jnp.int32, (cap, cap), 1)
        even, odd = wgot[k, 0:1, :cap], wgot[k, 1:2, :cap]
        mine = jnp.where(x == 0, even, odd)
        theirs = jnp.where(x == 0, odd, even)

        def column(row):
            return jnp.sum(jnp.where(d0 == d1, row, 0.0), axis=-1, keepdims=True)

        row = (
            column(mine) * vout[k, 0].astype(F32) + column(theirs) * vin[k].astype(F32)
        ).astype(BF16)
        if k == 0:
            back[z] = row
        else:
            ret[k] = row
            r_send(k).start()

    length = q_ref.shape[0]
    heads = q_ref.shape[1] // KEYDIM
    lead = heads // 2
    causal = (
        lax.broadcasted_iota(jnp.int32, (length, length), 1)
        <= lax.broadcasted_iota(jnp.int32, (length, length), 0)
    )

    def p_send(start):
        return remote(pay.at[pl.ds(start, lead)], payin, ps, pr, x_dev)

    def payload():
        floor_load.wait()
        f_load.wait()
        v_load.wait()
        tril = causal.astype(F32).astype(BF16)
        rates = (1.0 - floor_ref[...]) / (1.0 + jnp.exp(f_ref[...].astype(F32)))
        rate_ref[...] = rates
        cum = sum(
            jnp.dot(tril, piece, preferred_element_type=F32)
            for piece in split3(jnp.log(1.0 - rates))
        )
        cum_ref[...] = cum
        sub = lax.broadcasted_iota(jnp.int32, (PAD, KEYDIM), 0)
        for h in range(heads):
            at = slice(h * KEYDIM, (h + 1) * KEYDIM)
            end = cum[length - 1 : length, at]
            kend = (rates[:, at] * jnp.exp(end - cum[:, at])).astype(BF16)
            pay[h, :VDIM, :] = tn_dot(v_ref[:, at], kend).astype(BF16)
            high, mid, _ = split3(jnp.exp(end))
            pay[h, VDIM:, :] = jnp.where(
                sub == 0, high.astype(F32), jnp.where(sub == 1, mid.astype(F32), 0.0)
            ).astype(BF16)
        p_send((1 - x) * lead).start()

    def rest(h):
        at = slice(h * KEYDIM, (h + 1) * KEYDIM)
        cum = cum_ref[:, at]
        qexp = (silu(q_ref[:, at].astype(F32)) * jnp.exp(cum)).astype(BF16)
        kexp = (rate_ref[:, at] * jnp.exp(-cum)).astype(BF16)
        scores = jnp.where(causal, nt_dot(qexp, kexp), 0.0).astype(BF16)
        intra_ref[:, at] = jnp.dot(scores, v_ref[:, at], preferred_element_type=F32)
        qexp_ref[:, at] = qexp

    def pair_up():
        p_send(x * lead).wait_recv()
        for i in range(lead):
            mine = pay[x * lead + i].astype(F32)
            theirs = payin[i].astype(F32)
            s0 = jnp.where(x == 0, mine, theirs)
            s1 = jnp.where(x == 0, theirs, mine)
            d0 = s0[VDIM : VDIM + 1, :] + s0[VDIM + 1 : VDIM + 2, :]
            d1 = s1[VDIM : VDIM + 1, :] + s1[VDIM + 1 : VDIM + 2, :]
            sums[i] = d1 * s0[:VDIM, :] + s1[:VDIM, :]
            first[i] = s0[:VDIM, :]
            decays[i, 0:8] = jnp.broadcast_to(d0, (8, KEYDIM))
            decays[i, 8:16] = jnp.broadcast_to(d0 * d1, (8, KEYDIM))

    def h_send():
        return remote(chain_out, chain_in, hs, hr, device((z + 1) % GROUPS, x, y, c))

    def e_send(start):
        return remote(ent_out, ent.at[pl.ds(start, lead)], es, er, x_dev)

    def hop(step):
        @pl.when(z == step)
        def _():
            if step == 0:
                chain_in[...] = jnp.zeros_like(chain_in)
            else:
                h_send().wait_recv()
            if step < GROUPS - 1:
                for i in range(lead):
                    chain_out[i] = (
                        decays[i, 8:9] * chain_in[i].astype(F32) + sums[i]
                    ).astype(BF16)
                h_send().start()
            for i in range(lead):
                came = chain_in[i].astype(F32)
                later = decays[i, 0:1] * came + first[i]
                ent[x * lead + i] = jnp.where(x == 0, came, later).astype(BF16)
                ent_out[i] = jnp.where(x == 0, later, came).astype(BF16)
            e_send(x * lead).start()

    mix_rows = length // 2

    def m_send(j, at):
        ref = mix.at[at, pl.ds(j * mix_rows, mix_rows)]
        return remote(ref, ref, ms.at[j], mr.at[j], y_dev)

    def mc_send(j, at, n):
        ref = mix.at[at, pl.ds(j * mix_rows, mix_rows)]
        return remote(ref, ref, mcs.at[j, n], mcr.at[j, n], c_dev)

    def arrive_ent():
        e_send((1 - x) * lead).wait_recv()

    def finish(j):
        to = slice(j * mix_rows, (j + 1) * mix_rows)
        for h in range(heads):
            at = slice(h * VDIM, (h + 1) * VDIM)
            out = intra_ref[to, at] + nt_dot(qexp_ref[to, at], ent[h])
            norm = lax.rsqrt(jnp.mean(out * out, axis=-1, keepdims=True) + norm_eps)
            mix[own, to, at] = (
                out * norm * hgain_ref[...] * silu(g_ref[to, at].astype(F32))
            ).astype(BF16)
        m_send(j, own).start()
        mc_send(j, own, 0).start()

    def arrive_mix(j):
        m_send(j, quarter_y).wait_recv()
        mc_send(j, quarter_y, 1).start()

    def project(j):
        mc_send(j, quarter_c, 0).wait_recv()
        mc_send(j, quarter_d, 1).wait_recv()
        to = slice(j * mix_rows, (j + 1) * mix_rows)
        wide = proj_ref.shape[0] // 4
        mixer_ref[to, :] = sum(
            jnp.dot(mix[i, to, :], proj_ref[i * wide : (i + 1) * wide, :], preferred_element_type=F32)
            for i in range(4)
        ).astype(BF16)

    for k in (2, 1, 3):
        z_send(k).start()
    x_send(0, x).start()
    c_send(0, 0, c).start()
    for k in range(1, GROUPS):
        w_send(k).start()
    payload()
    q_load.wait()
    rest(0)
    rest(1)
    wg_load.wait()
    wu_load.wait()
    gate_up((0, 0))
    for h in range(2, heads):
        rest(h)
    arrive_z(2)
    arrive_x(0)
    pair_up()
    hop(0)
    arrive_y(0, 0)
    arrive_z(1)
    gate_up((0, 1))
    arrive_d(0)
    gate_up((1, 0))
    arrive_x(2)
    hop(1)
    gate_up((2, 0))
    arrive_y(0, 1)
    arrive_x(1)
    arrive_z(3)
    arrive_y(1, 0)
    arrive_d(1)
    gate_up((1, 1), (3, 0))
    wd_load.wait()
    down(0)
    hop(2)
    gate_up((2, 1))
    arrive_y(2, 0)
    arrive_x(3)
    arrive_y(1, 1)
    hop(3)
    arrive_y(3, 0)
    gate_up((3, 1))
    combine(0)
    arrive_y(2, 1)
    down(1)
    arrive_ent()
    g_load.wait()
    hgain_load.wait()
    finish(0)
    finish(1)
    down(2)
    combine(1)
    arrive_y(3, 1)
    combine(2)
    down(3)
    arrive_mix(0)
    proj_load.wait()
    combine(3)
    project(0)
    arrive_mix(1)
    project(1)
    for k in range(1, GROUPS):
        r_send(k).wait_recv()
    expert_ref[...] = tn_dot(perm[...], back[...].reshape(slots, back.shape[2])).astype(BF16)

    for k in range(GROUPS):
        if k > 0:
            z_send(k).wait_send()
            w_send(k).wait_send()
            r_send(k).wait_send()
        x_send(k, x).wait_send()
        v_send(k).wait_send()
        for i in range(2):
            c_send(k, i, c).wait_send()
            y_send(k, i, own).wait_send()
            hc_send(k, i, own, 0).wait_send()
            hc_send(k, i, quarter_y, 1).wait_send()
    for i in range(2):
        d_send(i, my_cols).wait_send()
        m_send(i, own).wait_send()
        mc_send(i, own, 0).wait_send()
        mc_send(i, quarter_y, 1).wait_send()
    p_send((1 - x) * lead).wait_send()
    e_send(x * lead).wait_send()

    @pl.when(z < GROUPS - 1)
    def _():
        h_send().wait_send()


def emit_kernel(mixer_ref, expert_ref, mixer_out, expert_out, sem):
    copies = [
        pltpu.make_async_copy(mixer_ref, mixer_out, sem.at[0]),
        pltpu.make_async_copy(expert_ref, expert_out, sem.at[1]),
    ]
    for copy in copies:
        copy.start()
    for copy in copies:
        copy.wait()


def fused(
    mixer_query, mixer_forget, mixer_value, mixer_gate, forget_floor, head_gain, mixer_proj,
    expert_tokens, expert_gain, routes, group_logits, choice_logits, w_gate, w_up, w_down,
):
    length, width = mixer_query.shape
    heads = width // KEYDIM
    lead = heads // 2
    experts = lax.axis_size("ep")
    rows, model = expert_tokens.shape
    cap = 2 * TOPK * rows // experts
    part = model // 2
    hidden = w_gate.shape[2]
    outs = w_down.shape[2]
    dma, n = pltpu.SemaphoreType.DMA, GROUPS
    any_spec = pl.BlockSpec(memory_space=pl.ANY)
    vmem = pltpu.VMEM
    mixer_out, expert_out = pl.pallas_call(
        fused_kernel,
        name="fused",
        out_shape=(
            vmem((length, mixer_proj.shape[1]), BF16),
            vmem((rows, outs), BF16),
        ),
        in_specs=[any_spec] * 15,
        out_specs=(VM, VM),
        scratch_shapes=[
            vmem((TOPK, rows), jnp.int32), vmem((GROUPS, rows), F32), vmem((TOPK, rows), F32),
            vmem((1, width), F32), vmem((1, VDIM), F32), vmem((1, model), F32),
            vmem((length, width), BF16), vmem((length, width), BF16),
            vmem((length, width), BF16), vmem((length, width), BF16),
            vmem((rows, model), BF16),
            vmem((model, hidden), BF16), vmem((model, hidden), BF16),
            vmem(w_down.shape[1:], BF16), vmem(mixer_proj.shape, BF16),
            vmem((n, cap, part), BF16),
            vmem((n, 8, 128), F32), vmem((n, 8, 128), F32),
            vmem((n, 2, 2, cap, part), BF16),
            vmem((n, 2, 4, cap, hidden), BF16),
            vmem((n, 2, cap, outs), BF16), vmem((n, cap, outs), BF16),
            vmem((n, cap, outs), BF16), vmem((n, cap, outs), BF16),
            vmem((n * cap, rows), BF16),
            vmem((length, width), F32), vmem((length, width), F32),
            vmem((length, width), BF16), vmem((length, width), F32),
            vmem((heads, VDIM + PAD, KEYDIM), BF16), vmem((lead, VDIM + PAD, KEYDIM), BF16),
            vmem((lead, VDIM, KEYDIM), F32), vmem((lead, 16, KEYDIM), F32),
            vmem((lead, VDIM, KEYDIM), F32),
            vmem((lead, VDIM, KEYDIM), BF16), vmem((lead, VDIM, KEYDIM), BF16),
            vmem((heads, VDIM, KEYDIM), BF16), vmem((lead, VDIM, KEYDIM), BF16),
            vmem((4, length, width), BF16),
            dma((15,)), dma((n,)), dma((n,)), dma((n,)), dma((n,)), dma((n,)), dma((n,)),
            dma((n, 2)), dma((n, 2)), dma((n, 2)), dma((n, 2)), dma((n, 2, 2)), dma((n, 2, 2)),
            dma((n,)), dma((n,)), dma((n,)), dma((n,)),
            dma, dma, dma, dma, dma, dma, dma((2,)), dma((2,)), dma((2, 2)), dma((2, 2)),
            dma((2,)), dma((2,)),
        ],
        compiler_params=pltpu.CompilerParams(
            collective_id=0, has_side_effects=True, vmem_limit_bytes=64000000
        ),
        cost_estimate=cost(8000000000, 12000000),
    )(
        routes.T, group_logits.T, choice_logits.T, forget_floor[None, :], head_gain[None, :],
        expert_gain[None, :], mixer_query, mixer_forget, mixer_value, mixer_gate,
        expert_tokens, w_gate[0], w_up[0], w_down[0], mixer_proj,
    )
    return pl.pallas_call(
        emit_kernel,
        name="emit",
        out_shape=(shaped(mixer_out.shape, BF16), shaped(expert_out.shape, BF16)),
        in_specs=[any_spec, any_spec],
        out_specs=(any_spec, any_spec),
        scratch_shapes=[dma((2,))],
        compiler_params=pltpu.CompilerParams(vmem_limit_bytes=1000000),
        cost_estimate=cost(1000000, 800000),
    )(mixer_out, expert_out)


def per_device(
    mixer_query, mixer_forget, mixer_value, mixer_gate, forget_floor, head_gain, mixer_proj,
    expert_tokens, expert_gain, routes, group_logits, choice_logits, w_gate, w_up, w_down,
):
    length, width = mixer_query.shape
    heads = width // KEYDIM
    experts = lax.axis_size("ep")
    tp = lax.axis_size("tp")
    rows, model = expert_tokens.shape
    capacity = 2 * TOPK * rows // experts
    slots = experts * capacity
    split = 2
    part = model // split
    which = lax.axis_index("tp") % split
    half = jnp.full((experts + 1,), 0, jnp.int32) + which

    outgoing, wt = pl.pallas_call(
        dispatch_kernel,
        name="dispatch",
        out_shape=(shaped((slots, part), BF16), shaped((2, rows, slots), BF16)),
        in_specs=[SM, VM, VM, VM, VM, VM],
        out_specs=(VM, VM),
        cost_estimate=cost(2 * rows * slots * part, 4000000),
    )(half, expert_tokens, expert_gain[None, :], routes.T, group_logits.T, choice_logits.T)
    arrived = lax.all_to_all(
        outgoing.reshape(experts, capacity, part), "ep", split_axis=0, concat_axis=0, tiled=True
    )

    intra, qexp, pay = pl.pallas_call(
        local_kernel,
        name="local_scan",
        out_shape=(
            shaped((length, width), F32),
            shaped((length, width), BF16),
            shaped((heads, VDIM + PAD, KEYDIM), BF16),
        ),
        in_specs=[VM] * 4,
        out_specs=(VM, VM, VM),
        cost_estimate=cost(3000000000, 4000000),
    )(mixer_query, mixer_forget, mixer_value, forget_floor[None, :])
    arrived, pay = lax.optimization_barrier((arrived, pay))
    entering = prefix(pay, experts)
    mixed = pl.pallas_call(
        finish_kernel,
        name="mixer_finish",
        out_shape=shaped((length, width), BF16),
        in_specs=[VM] * 5,
        out_specs=VM,
        cost_estimate=cost(1000000000, 4000000),
    )(entering, intra, qexp, mixer_gate, head_gain[None, :])
    mixed_all = lax.all_gather(mixed, "tp", axis=1, tiled=True)

    own = arrived.reshape(slots, part)
    other = lax.ppermute(own, "tp", [(i, i ^ 1) for i in range(tp)])
    flat_in = jnp.concatenate(
        [jnp.where(which == 0, own, other), jnp.where(which == 0, other, own)], axis=1
    )
    gate_pre = jnp.dot(flat_in, w_gate[0], preferred_element_type=F32)
    up_pre = jnp.dot(flat_in, w_up[0], preferred_element_type=F32)
    hidden = (jax.nn.silu(gate_pre) * up_pre).astype(BF16)
    hidden_all = lax.all_gather(hidden, "tp", axis=1, tiled=True)
    mixer_out = jnp.dot(mixed_all, mixer_proj, preferred_element_type=F32).astype(BF16)
    down = jnp.dot(hidden_all, w_down[0], preferred_element_type=F32).astype(BF16)
    back = lax.all_to_all(
        down.reshape(experts, capacity, -1), "ep", split_axis=0, concat_axis=0, tiled=True
    ).reshape(slots, -1)
    expert_out = pl.pallas_call(
        return_kernel,
        name="weigh",
        out_shape=shaped((rows, back.shape[1]), BF16),
        in_specs=[VM, VM],
        out_specs=VM,
        cost_estimate=cost(4 * rows * slots * back.shape[1], 1000000),
    )(wt, back)
    return (mixer_out, expert_out)


def solution(mesh):
    paired = mesh.shape["ep"] == GROUPS * TOPK and mesh.shape["tp"] == 4
    return jax.shard_map(
        fused if paired else per_device,
        mesh=mesh,
        in_specs=(
            P("ep", "tp"),
            P("ep", "tp"),
            P("ep", "tp"),
            P("ep", "tp"),
            P("tp"),
            P(),
            P(None, "tp"),
            P("ep", None),
            P(),
            P("ep", None),
            P("ep", None),
            P("ep", None),
            P("ep", None, "tp"),
            P("ep", None, "tp"),
            P("ep", None, "tp"),
        ),
        out_specs=(P("ep", "tp"), P("ep", "tp")),
        check_vma=False,
    )
```

```python
import jax
import jax.numpy as jnp
from jax import lax
from jax.experimental import pallas as pl
from jax.experimental.pallas import tpu as pltpu
from jax.sharding import PartitionSpec as P

KEYDIM = 128
VDIM = 128
GROUPS = 4
TOPK = 2
SPLIT = 2
PAD = 16
norm_eps = 1e-06
F32 = jnp.float32
BF16 = jnp.bfloat16
VM = pl.BlockSpec(memory_space=pltpu.VMEM)
SM = pl.BlockSpec(memory_space=pltpu.SMEM)


def tn_dot(a, b):
    return lax.dot_general(a, b, (((0,), (0,)), ((), ())), preferred_element_type=F32)


def nt_dot(a, b):
    return lax.dot_general(a, b, (((1,), (1,)), ((), ())), preferred_element_type=F32)


def silu(v):
    return v / (1.0 + jnp.exp(-v))


def local_kernel(q_ref, f_ref, v_ref, floor_ref, intra_ref, qexp_ref, pay_ref):
    length = q_ref.shape[0]
    rows = lax.broadcasted_iota(jnp.int32, (length, length), 0)
    cols = lax.broadcasted_iota(jnp.int32, (length, length), 1)
    causal = cols <= rows
    tril = causal.astype(F32)
    for h in range(q_ref.shape[1] // KEYDIM):
        at = slice(h * KEYDIM, (h + 1) * KEYDIM)
        floor = floor_ref[:, at]
        rates = (1.0 - floor) / (1.0 + jnp.exp(f_ref[:, at].astype(F32)))
        cum = jnp.dot(
            tril, jnp.log(1.0 - rates), precision=lax.Precision.HIGHEST,
            preferred_element_type=F32,
        )
        end = cum[length - 1 : length, :]
        qexp = (silu(q_ref[:, at].astype(F32)) * jnp.exp(cum)).astype(BF16)
        kexp = (rates * jnp.exp(-cum)).astype(BF16)
        kend = (rates * jnp.exp(end - cum)).astype(BF16)
        value = v_ref[:, at]
        scores = jnp.where(causal, nt_dot(qexp, kexp), 0.0).astype(BF16)
        intra_ref[:, at] = jnp.dot(scores, value, preferred_element_type=F32)
        qexp_ref[:, at] = qexp
        pay_ref[h, :VDIM, :] = tn_dot(value, kend).astype(BF16)
        pay_ref[h, VDIM:, :] = jnp.broadcast_to(jnp.exp(end), (PAD, KEYDIM)).astype(BF16)


def finish_kernel(state_ref, intra_ref, qexp_ref, gate_ref, gain_ref, out_ref):
    for h in range(intra_ref.shape[1] // VDIM):
        at = slice(h * VDIM, (h + 1) * VDIM)

        out = intra_ref[:, at] + nt_dot(qexp_ref[:, at], state_ref[h, :VDIM, :])
        scale = lax.rsqrt(jnp.mean(out * out, axis=-1, keepdims=True) + norm_eps)
        out_ref[:, at] = (
            out * scale * gain_ref[...] * silu(gate_ref[:, at].astype(F32))
        ).astype(BF16)


def dispatch_kernel(half_ref, x_ref, gain_ref, routes_ref, gl_ref, cl_ref, out_ref, wt_ref):
    rows, width = x_ref.shape
    slots = out_ref.shape[0]
    part = out_ref.shape[1]
    experts = half_ref.shape[0] - 1
    capacity = slots // experts
    group_size = experts // GROUPS
    t0 = lax.broadcasted_iota(jnp.int32, (rows, rows), 0)
    t1 = lax.broadcasted_iota(jnp.int32, (rows, rows), 1)

    def column(row):
        return jnp.sum(jnp.where(t0 == t1, row.astype(F32), 0.0), axis=-1, keepdims=True)

    route = [column(routes_ref[j : j + 1, :]).astype(jnp.int32) for j in range(TOPK)]
    ids = lax.broadcasted_iota(jnp.int32, (rows, experts), 1)
    hot = [(r == ids).astype(F32) for r in route]
    before = jnp.dot(
        (t1 < t0).astype(BF16), sum(hot).astype(BF16), preferred_element_type=F32
    )
    group_exp = [jnp.exp(column(gl_ref[g : g + 1, :])) for g in range(GROUPS)]
    group_sum = sum(group_exp)
    gids = lax.broadcasted_iota(jnp.int32, (rows, GROUPS), 1)
    member = [
        ((r >= gids * group_size) & (r < (gids + 1) * group_size)).astype(F32) for r in route
    ]
    choice = [jnp.exp(column(cl_ref[j : j + 1, :])) for j in range(TOPK)]
    slot_ids = lax.broadcasted_iota(jnp.int32, (rows, slots), 1)
    place = jnp.zeros((rows, slots), F32)
    weight = jnp.zeros((rows, slots), F32)
    for j in range(TOPK):
        rank = jnp.sum(before * hot[j], axis=-1, keepdims=True).astype(jnp.int32)
        mark = (slot_ids == route[j] * capacity + rank).astype(F32)
        within = sum(
            jnp.sum(member[j] * member[i], axis=-1, keepdims=True) * choice[i]
            for i in range(TOPK)
        )
        prob = sum(member[j][:, g : g + 1] * group_exp[g] for g in range(GROUPS)) / group_sum
        place = place + mark
        weight = weight + mark * (prob * choice[j] / within)
    high = weight.astype(BF16)
    wt_ref[0] = high
    wt_ref[1] = (weight - high.astype(F32)).astype(BF16)
    x = x_ref[...].astype(F32)
    scale = lax.rsqrt(jnp.mean(x * x, axis=-1, keepdims=True) + norm_eps)
    cols = pl.ds(pl.multiple_of(half_ref[0] * part, part), part)
    normed = (x_ref[:, cols].astype(F32) * scale * gain_ref[:, cols]).astype(BF16)
    out_ref[...] = tn_dot(place.astype(BF16), normed).astype(BF16)


def return_kernel(wt_ref, back_ref, out_ref):
    back = back_ref[...]
    out_ref[...] = (
        jnp.dot(wt_ref[0], back, preferred_element_type=F32)
        + jnp.dot(wt_ref[1], back, preferred_element_type=F32)
    ).astype(BF16)


def later_after(later, earlier):
    later = later.astype(F32)
    rows = lax.broadcasted_iota(jnp.int32, later.shape, 1)
    decay = later[:, VDIM : VDIM + 1, :]
    return (decay * earlier.astype(F32) + jnp.where(rows < VDIM, later, 0.0)).astype(BF16)


def prefix(pay, count):
    span = pay
    before = None
    step = 1
    while step < count:
        came = lax.ppermute(span, "ep", [(i, i + step) for i in range(count - step)])
        before = came if before is None else later_after(before, came)
        step *= 2
        if step < count:
            span = later_after(span, came)
    return jnp.zeros_like(pay) if before is None else before


def cost(flops, size):
    return pl.CostEstimate(flops=flops, bytes_accessed=size, transcendentals=0)


def shaped(shape, kind):
    return jax.ShapeDtypeStruct(shape, kind)


def remote(src, dst, send, recv, device):
    return pltpu.make_async_remote_copy(
        src_ref=src, dst_ref=dst, send_sem=send, recv_sem=recv, device_id=device,
        device_id_type=pl.DeviceIdType.MESH,
    )


def other_plane(z, k):
    return (z % 2 + k % 2) % 2 + 2 * ((z // 2 + k // 2) % 2)


def split3(v):
    high = v.astype(BF16)
    rest = v - high.astype(F32)
    mid = rest.astype(BF16)
    return high, mid, (rest - mid.astype(F32)).astype(BF16)


def fused_kernel(
    routes_hbm, gl_hbm, cl_hbm, floor_hbm, hgain_hbm, egain_hbm,
    q_hbm, f_hbm, v_hbm, g_hbm, tok_hbm, wg_hbm, wu_hbm, wd_hbm, proj_hbm,
    mixer_ref, expert_ref,
    routes_ref, gl_ref, cl_ref, floor_ref, hgain_ref, egain_ref,
    q_ref, f_ref, v_ref, g_ref, tok_ref, wg_ref, wu_ref, wd_ref, proj_ref,
    disp, wsrc, wgot, flat, hid, vout, vin, ret, back, perm,
    cum_ref, rate_ref, qexp_ref, intra_ref, pay, payin, sums, decays, first, chain_in, chain_out,
    ent, ent_out, mix,
    load_sem, zs, zr, ws, wr, xs, xr, cs, cr, ys, yr, hcs, hcr, vs, vr, rs, rr,
    ps, pr, hs, hr, es, er, ms, mr, mcs, mcr, ds, dr,
):
    ep, tp = lax.axis_index("ep"), lax.axis_index("tp")
    z, x = ep // 2, ep % 2
    y, c = tp // 2, tp % 2
    own = tp
    quarter_y = (1 - y) * 2 + c
    quarter_c = y * 2 + (1 - c)
    quarter_d = (1 - y) * 2 + (1 - c)

    def device(z_, x_, y_, c_):
        return (z_ * 2 + x_, y_ * 2 + c_)

    x_dev = device(z, 1 - x, y, c)
    y_dev = device(z, x, 1 - y, c)
    c_dev = device(z, x, y, 1 - c)
    planes = [other_plane(z, k) for k in range(GROUPS)]
    z_dev = [device(p, x, y, c) for p in planes]

    loads = [
        pltpu.make_async_copy(src, dst, load_sem.at[i])
        for i, (src, dst) in enumerate([
            (routes_hbm, routes_ref), (gl_hbm, gl_ref), (cl_hbm, cl_ref),
            (tok_hbm, tok_ref), (egain_hbm, egain_ref), (floor_hbm, floor_ref), (f_hbm, f_ref), (v_hbm, v_ref), (q_hbm, q_ref),
            (wg_hbm, wg_ref), (wu_hbm, wu_ref), (g_hbm, g_ref), (wd_hbm, wd_ref),
            (proj_hbm, proj_ref), (hgain_hbm, hgain_ref),
        ])
    ]
    (
        routes_load, gl_load, cl_load, tok_load, egain_load, floor_load, f_load, v_load, q_load,
        wg_load, wu_load, g_load, wd_load, proj_load, hgain_load,
    ) = loads
    for load in loads:
        load.start()
    barrier = pltpu.get_barrier_semaphore()
    for dev in z_dev[1:] + [x_dev, y_dev, c_dev]:
        pl.semaphore_signal(
            barrier, inc=1, device_id=dev, device_id_type=pl.DeviceIdType.MESH
        )

    rows = tok_ref.shape[0]
    width = tok_ref.shape[1]
    cap, part = disp.shape[1], disp.shape[2]
    slots = GROUPS * cap
    group_size = TOPK
    routes_load.wait()
    route = [routes_ref[j : j + 1, :] for j in range(TOPK)]
    gids = lax.broadcasted_iota(jnp.int32, (8, rows), 0)
    member = [
        ((r >= gids * group_size) & (r < (gids + 1) * group_size)).astype(F32) for r in route
    ]
    t0 = lax.broadcasted_iota(jnp.int32, (rows, rows), 0)
    t1 = lax.broadcasted_iota(jnp.int32, (rows, rows), 1)
    before = jnp.dot(
        member[0].astype(BF16), (t0 < t1).astype(BF16), preferred_element_type=F32
    )

    def over_groups(v):
        return jnp.sum(v, axis=0, keepdims=True)

    rank = over_groups(before * member[0]).astype(jnp.int32)
    group = over_groups(gids.astype(F32) * member[0]).astype(jnp.int32)
    slot_ids = lax.broadcasted_iota(jnp.int32, (slots, rows), 0)
    perm[...] = (slot_ids == group * cap + rank).astype(F32).astype(BF16)

    tok_load.wait()
    egain_load.wait()
    tokens = tok_ref[...].astype(F32)
    scale = lax.rsqrt(jnp.mean(tokens * tokens, axis=-1, keepdims=True) + norm_eps)
    cols = pl.ds(pl.multiple_of(c * part, part), part)
    normed = (tok_ref[:, cols].astype(F32) * scale * egain_ref[:, cols]).astype(BF16)
    for i in range(GROUPS):
        chosen = perm[i * cap : (i + 1) * cap, :]
        disp[i] = jnp.dot(chosen, normed, preferred_element_type=F32).astype(BF16)
    flat[0, c, x] = disp[z]

    pl.semaphore_wait(barrier, len(z_dev[1:]) + 3)

    half_part = part // 2
    my_cols = pl.ds(pl.multiple_of(y * half_part, half_part), half_part)
    other_cols = pl.ds(pl.multiple_of((1 - y) * half_part, half_part), half_part)
    block = [x, 1 - x]

    def piece(k, b, at=my_cols):
        return flat.at[k, c, b, :, at] if k == SPLIT else flat.at[k, c, b]

    def z_send(k):
        rows_of = disp.at[planes[k], :, my_cols] if k == SPLIT else disp.at[planes[k]]
        return remote(rows_of, piece(k, x), zs.at[k], zr.at[k], z_dev[k])

    def w_send(k):
        return remote(wsrc.at[planes[k]], wgot.at[k], ws.at[k], wr.at[k], z_dev[k])

    def x_send(k, b):
        return remote(piece(k, b), piece(k, b), xs.at[k], xr.at[k], x_dev)

    def d_send(i, at):
        ref = piece(SPLIT, block[i], at)
        return remote(ref, ref, ds.at[i], dr.at[i], y_dev)

    def c_send(k, i, half):
        ref = flat.at[k, half, block[i]]
        return remote(ref, ref, cs.at[k, i], cr.at[k, i], c_dev)

    def arrive_z(k):
        z_send(k).wait_recv()
        x_send(k, x).start()
        if k == SPLIT:
            d_send(0, my_cols).start()
        else:
            c_send(k, 0, c).start()

    def arrive_x(k):
        x_send(k, 1 - x).wait_recv()
        if k == SPLIT:
            d_send(1, my_cols).start()
        else:
            c_send(k, 1, c).start()

    def arrive_d(i):
        d_send(i, other_cols).wait_recv()
        c_send(SPLIT, i, c).start()

    def y_send(k, i, at):
        ref = hid.at[k, block[i], at]
        return remote(ref, ref, ys.at[k, i], yr.at[k, i], y_dev)

    def hc_send(k, i, at, n):
        ref = hid.at[k, block[i], at]
        return remote(ref, ref, hcs.at[k, i, n], hcr.at[k, i, n], c_dev)

    def gate_up(*blocks):
        for k, i in blocks:
            c_send(k, i, 1 - c).wait_recv()
        a = [
            jnp.concatenate([flat[k, n, block[i]] for k, i in blocks], axis=0) for n in range(2)
        ]
        gate = sum(
            jnp.dot(a[n], wg_ref[n * part : (n + 1) * part, :], preferred_element_type=F32)
            for n in range(2)
        )
        up = sum(
            jnp.dot(a[n], wu_ref[n * part : (n + 1) * part, :], preferred_element_type=F32)
            for n in range(2)
        )
        act = (silu(gate) * up).astype(BF16)
        for m, (k, i) in enumerate(blocks):
            hid[k, block[i], own] = act[m * cap : (m + 1) * cap]
            y_send(k, i, own).start()
            hc_send(k, i, own, 0).start()

    def arrive_y(k, i):
        y_send(k, i, quarter_y).wait_recv()
        hc_send(k, i, quarter_y, 1).start()

    depth = wd_ref.shape[0] // 4

    def pieces(k):
        count = 2 if k == GROUPS - 1 else 1
        size = vout.shape[3] // count
        return [slice(j * size, (j + 1) * size) for j in range(count)]

    def v_send(k, j):
        at = pieces(k)[j]
        return remote(vout.at[k, 1, :, at], vin.at[k, :, at], vs.at[k, j], vr.at[k, j], x_dev)

    def down(k):
        for i in range(2):
            hc_send(k, i, quarter_c, 0).wait_recv()
            hc_send(k, i, quarter_d, 1).wait_recv()
        act = [jnp.concatenate([hid[k, block[i], n] for i in range(2)], axis=0) for n in range(4)]
        for j, at in enumerate(pieces(k)):
            value = sum(
                jnp.dot(
                    act[n], wd_ref[n * depth : (n + 1) * depth, at], preferred_element_type=F32
                )
                for n in range(4)
            ).astype(BF16)
            vout[k, 0, :, at] = value[:cap]
            vout[k, 1, :, at] = value[cap:]
            v_send(k, j).start()

    def r_send(k, j):
        at = pieces(k)[j]
        return remote(ret.at[k, :, at], back.at[z, :, at], rs.at[k, j], rr.at[k, j], z_dev[k])

    def combine(k, j=0):
        v_send(k, j).wait_recv()
        if k > 0 and j == 0:
            w_send(k).wait_recv()
        d0 = lax.broadcasted_iota(jnp.int32, (cap, cap), 0)
        d1 = lax.broadcasted_iota(jnp.int32, (cap, cap), 1)
        even, odd = wgot[k, 0:1, :cap], wgot[k, 1:2, :cap]
        mine = jnp.where(x == 0, even, odd)
        theirs = jnp.where(x == 0, odd, even)

        def column(row):
            return jnp.sum(jnp.where(d0 == d1, row, 0.0), axis=-1, keepdims=True)

        at = pieces(k)[j]
        row = (
            column(mine) * vout[k, 0, :, at].astype(F32)
            + column(theirs) * vin[k, :, at].astype(F32)
        ).astype(BF16)
        if k == 0:
            back[z] = row
        else:
            ret[k, :, at] = row
            r_send(k, j).start()

    def weights():
        gl_load.wait()
        cl_load.wait()
        group_exp = [jnp.exp(gl_ref[i : i + 1, :]) for i in range(GROUPS)]
        group_sum = sum(group_exp)
        choice = [jnp.exp(cl_ref[j : j + 1, :]) for j in range(TOPK)]
        expert_weight = [0.0] * group_size
        for j in range(TOPK):
            within = sum(over_groups(member[j] * member[i]) * choice[i] for i in range(TOPK))
            prob = sum(member[j][i : i + 1, :] * group_exp[i] for i in range(GROUPS)) / group_sum
            weight = prob * choice[j] / within
            for m in range(group_size):
                named = route[j] == group * group_size + m
                expert_weight[m] = expert_weight[m] + jnp.where(named, weight, 0.0)
        sub = lax.broadcasted_iota(jnp.int32, (8, rows), 0)
        stacked = jnp.zeros((8, rows), F32)
        for m in range(group_size):
            for i, piece in enumerate(split3(expert_weight[m])):
                stacked = jnp.where(sub == 3 * m + i, piece.astype(F32), stacked)
        stacked = stacked.astype(BF16)
        for i in range(GROUPS):
            chosen = perm[i * cap : (i + 1) * cap, :]
            got = nt_dot(stacked, chosen)
            pair = [got[3 * m : 3 * m + 1, :] + got[3 * m + 1 : 3 * m + 2, :] + got[3 * m + 2 : 3 * m + 3, :]
                    for m in range(group_size)]
            lanes = lax.broadcasted_iota(jnp.int32, (8, cap), 0)
            packed = jnp.where(lanes == 0, pair[0], jnp.where(lanes == 1, pair[1], 0.0))
            wsrc[i] = jnp.concatenate([packed, jnp.zeros((8, wsrc.shape[2] - cap), F32)], axis=1)
        wgot[0] = wsrc[z]
        for k in range(1, GROUPS):
            w_send(k).start()

    length = q_ref.shape[0]
    heads = q_ref.shape[1] // KEYDIM
    lead = heads // 2
    causal = (
        lax.broadcasted_iota(jnp.int32, (length, length), 1)
        <= lax.broadcasted_iota(jnp.int32, (length, length), 0)
    )

    def p_send(start):
        return remote(pay.at[pl.ds(start, lead)], payin, ps, pr, x_dev)

    def payload():
        floor_load.wait()
        f_load.wait()
        v_load.wait()
        tril = causal.astype(F32).astype(BF16)
        rates = (1.0 - floor_ref[...]) / (1.0 + jnp.exp(f_ref[...].astype(F32)))
        rate_ref[...] = rates
        cum = sum(
            jnp.dot(tril, piece, preferred_element_type=F32)
            for piece in split3(jnp.log(1.0 - rates))
        )
        cum_ref[...] = cum
        sub = lax.broadcasted_iota(jnp.int32, (PAD, KEYDIM), 0)
        for h in range(heads):
            at = slice(h * KEYDIM, (h + 1) * KEYDIM)
            end = cum[length - 1 : length, at]
            kend = (rates[:, at] * jnp.exp(end - cum[:, at])).astype(BF16)
            pay[h, :VDIM, :] = tn_dot(v_ref[:, at], kend).astype(BF16)
            high, mid, _ = split3(jnp.exp(end))
            pay[h, VDIM:, :] = jnp.where(
                sub == 0, high.astype(F32), jnp.where(sub == 1, mid.astype(F32), 0.0)
            ).astype(BF16)
        p_send((1 - x) * lead).start()

    def rest(h):
        at = slice(h * KEYDIM, (h + 1) * KEYDIM)
        cum = cum_ref[:, at]
        qexp = (silu(q_ref[:, at].astype(F32)) * jnp.exp(cum)).astype(BF16)
        kexp = (rate_ref[:, at] * jnp.exp(-cum)).astype(BF16)
        scores = jnp.where(causal, nt_dot(qexp, kexp), 0.0).astype(BF16)
        intra_ref[:, at] = jnp.dot(scores, v_ref[:, at], preferred_element_type=F32)
        qexp_ref[:, at] = qexp

    def pair_up():
        p_send(x * lead).wait_recv()
        for i in range(lead):
            mine = pay[x * lead + i].astype(F32)
            theirs = payin[i].astype(F32)
            s0 = jnp.where(x == 0, mine, theirs)
            s1 = jnp.where(x == 0, theirs, mine)
            d0 = s0[VDIM : VDIM + 1, :] + s0[VDIM + 1 : VDIM + 2, :]
            d1 = s1[VDIM : VDIM + 1, :] + s1[VDIM + 1 : VDIM + 2, :]
            sums[i] = d1 * s0[:VDIM, :] + s1[:VDIM, :]
            first[i] = s0[:VDIM, :]
            decays[i, 0:8] = jnp.broadcast_to(d0, (8, KEYDIM))
            decays[i, 8:16] = jnp.broadcast_to(d0 * d1, (8, KEYDIM))

    def h_send():
        return remote(chain_out, chain_in, hs, hr, device((z + 1) % GROUPS, x, y, c))

    def e_send(start):
        return remote(ent_out, ent.at[pl.ds(start, lead)], es, er, x_dev)

    def hop(step):
        @pl.when(z == step)
        def _():
            if step == 0:
                chain_in[...] = jnp.zeros_like(chain_in)
            else:
                h_send().wait_recv()
            if step < GROUPS - 1:
                for i in range(lead):
                    chain_out[i] = (
                        decays[i, 8:9] * chain_in[i].astype(F32) + sums[i]
                    ).astype(BF16)
                h_send().start()
            for i in range(lead):
                came = chain_in[i].astype(F32)
                later = decays[i, 0:1] * came + first[i]
                ent[x * lead + i] = jnp.where(x == 0, came, later).astype(BF16)
                ent_out[i] = jnp.where(x == 0, later, came).astype(BF16)
            e_send(x * lead).start()

    mix_rows = length // 2

    def m_send(j, at):
        ref = mix.at[at, pl.ds(j * mix_rows, mix_rows)]
        return remote(ref, ref, ms.at[j], mr.at[j], y_dev)

    def mc_send(j, at, n):
        ref = mix.at[at, pl.ds(j * mix_rows, mix_rows)]
        return remote(ref, ref, mcs.at[j, n], mcr.at[j, n], c_dev)

    def arrive_ent():
        e_send((1 - x) * lead).wait_recv()

    def finish(j):
        to = slice(j * mix_rows, (j + 1) * mix_rows)
        for h in range(heads):
            at = slice(h * VDIM, (h + 1) * VDIM)
            out = intra_ref[to, at] + nt_dot(qexp_ref[to, at], ent[h])
            norm = lax.rsqrt(jnp.mean(out * out, axis=-1, keepdims=True) + norm_eps)
            mix[own, to, at] = (
                out * norm * hgain_ref[...] * silu(g_ref[to, at].astype(F32))
            ).astype(BF16)
        m_send(j, own).start()
        mc_send(j, own, 0).start()

    def arrive_mix(j):
        m_send(j, quarter_y).wait_recv()
        mc_send(j, quarter_y, 1).start()

    def project(j):
        mc_send(j, quarter_c, 0).wait_recv()
        mc_send(j, quarter_d, 1).wait_recv()
        to = slice(j * mix_rows, (j + 1) * mix_rows)
        wide = proj_ref.shape[0] // 4
        mixer_ref[to, :] = sum(
            jnp.dot(mix[i, to, :], proj_ref[i * wide : (i + 1) * wide, :], preferred_element_type=F32)
            for i in range(4)
        ).astype(BF16)

    for k in (2, 1, 3):
        z_send(k).start()
    x_send(0, x).start()
    c_send(0, 0, c).start()
    payload()
    weights()
    q_load.wait()
    rest(0)
    rest(1)
    wg_load.wait()
    wu_load.wait()
    gate_up((0, 0))
    for h in range(2, heads):
        rest(h)
    arrive_z(2)
    arrive_x(0)
    pair_up()
    hop(0)
    arrive_y(0, 0)
    arrive_z(1)
    gate_up((0, 1))
    arrive_d(0)
    arrive_x(2)
    gate_up((2, 0), (1, 0))
    arrive_z(3)
    hop(1)
    arrive_x(1)
    arrive_y(0, 1)
    gate_up((3, 0))
    arrive_d(1)
    wd_load.wait()
    down(0)
    gate_up((2, 1))
    arrive_x(3)
    hop(2)
    arrive_y(2, 0)
    arrive_y(1, 0)
    gate_up((3, 1), (1, 1))
    hop(3)
    arrive_y(3, 0)
    arrive_y(2, 1)
    combine(0)
    arrive_ent()
    g_load.wait()
    hgain_load.wait()
    finish(0)
    down(2)
    finish(1)
    arrive_y(3, 1)
    arrive_y(1, 1)
    down(3)
    down(1)
    combine(2)
    arrive_mix(0)
    combine(3, 0)
    combine(3, 1)
    combine(1)
    arrive_mix(1)
    proj_load.wait()
    project(0)
    project(1)
    for k in range(1, GROUPS):
        for j in range(len(pieces(k))):
            r_send(k, j).wait_recv()
    expert_ref[...] = tn_dot(perm[...], back[...].reshape(slots, back.shape[2])).astype(BF16)

    for k in range(GROUPS):
        if k > 0:
            z_send(k).wait_send()
            w_send(k).wait_send()
            for j in range(len(pieces(k))):
                r_send(k, j).wait_send()
        x_send(k, x).wait_send()
        for j in range(len(pieces(k))):
            v_send(k, j).wait_send()
        for i in range(2):
            c_send(k, i, c).wait_send()
            y_send(k, i, own).wait_send()
            hc_send(k, i, own, 0).wait_send()
            hc_send(k, i, quarter_y, 1).wait_send()
    for i in range(2):
        d_send(i, my_cols).wait_send()
        m_send(i, own).wait_send()
        mc_send(i, own, 0).wait_send()
        mc_send(i, quarter_y, 1).wait_send()
    p_send((1 - x) * lead).wait_send()
    e_send(x * lead).wait_send()

    @pl.when(z < GROUPS - 1)
    def _():
        h_send().wait_send()


def emit_kernel(mixer_ref, expert_ref, mixer_out, expert_out, sem):
    copies = [
        pltpu.make_async_copy(mixer_ref, mixer_out, sem.at[0]),
        pltpu.make_async_copy(expert_ref, expert_out, sem.at[1]),
    ]
    for copy in copies:
        copy.start()
    for copy in copies:
        copy.wait()


def fused(
    mixer_query, mixer_forget, mixer_value, mixer_gate, forget_floor, head_gain, mixer_proj,
    expert_tokens, expert_gain, routes, group_logits, choice_logits, w_gate, w_up, w_down,
):
    length, width = mixer_query.shape
    heads = width // KEYDIM
    lead = heads // 2
    experts = lax.axis_size("ep")
    rows, model = expert_tokens.shape
    cap = 2 * TOPK * rows // experts
    part = model // 2
    hidden = w_gate.shape[2]
    outs = w_down.shape[2]
    dma, n = pltpu.SemaphoreType.DMA, GROUPS
    any_spec = pl.BlockSpec(memory_space=pl.ANY)
    vmem = pltpu.VMEM
    mixer_out, expert_out = pl.pallas_call(
        fused_kernel,
        name="fused",
        out_shape=(
            vmem((length, mixer_proj.shape[1]), BF16),
            vmem((rows, outs), BF16),
        ),
        in_specs=[any_spec] * 15,
        out_specs=(VM, VM),
        scratch_shapes=[
            vmem((TOPK, rows), jnp.int32), vmem((GROUPS, rows), F32), vmem((TOPK, rows), F32),
            vmem((1, width), F32), vmem((1, VDIM), F32), vmem((1, model), F32),
            vmem((length, width), BF16), vmem((length, width), BF16),
            vmem((length, width), BF16), vmem((length, width), BF16),
            vmem((rows, model), BF16),
            vmem((model, hidden), BF16), vmem((model, hidden), BF16),
            vmem(w_down.shape[1:], BF16), vmem(mixer_proj.shape, BF16),
            vmem((n, cap, part), BF16),
            vmem((n, 8, 128), F32), vmem((n, 8, 128), F32),
            vmem((n, 2, 2, cap, part), BF16),
            vmem((n, 2, 4, cap, hidden), BF16),
            vmem((n, 2, cap, outs), BF16), vmem((n, cap, outs), BF16),
            vmem((n, cap, outs), BF16), vmem((n, cap, outs), BF16),
            vmem((n * cap, rows), BF16),
            vmem((length, width), F32), vmem((length, width), F32),
            vmem((length, width), BF16), vmem((length, width), F32),
            vmem((heads, VDIM + PAD, KEYDIM), BF16), vmem((lead, VDIM + PAD, KEYDIM), BF16),
            vmem((lead, VDIM, KEYDIM), F32), vmem((lead, 16, KEYDIM), F32),
            vmem((lead, VDIM, KEYDIM), F32),
            vmem((lead, VDIM, KEYDIM), BF16), vmem((lead, VDIM, KEYDIM), BF16),
            vmem((heads, VDIM, KEYDIM), BF16), vmem((lead, VDIM, KEYDIM), BF16),
            vmem((4, length, width), BF16),
            dma((15,)), dma((n,)), dma((n,)), dma((n,)), dma((n,)), dma((n,)), dma((n,)),
            dma((n, 2)), dma((n, 2)), dma((n, 2)), dma((n, 2)), dma((n, 2, 2)), dma((n, 2, 2)),
            dma((n, 2)), dma((n, 2)), dma((n, 2)), dma((n, 2)),
            dma, dma, dma, dma, dma, dma, dma((2,)), dma((2,)), dma((2, 2)), dma((2, 2)),
            dma((2,)), dma((2,)),
        ],
        compiler_params=pltpu.CompilerParams(
            collective_id=0, has_side_effects=True, vmem_limit_bytes=64000000
        ),
        cost_estimate=cost(8000000000, 12000000),
    )(
        routes.T, group_logits.T, choice_logits.T, forget_floor[None, :], head_gain[None, :],
        expert_gain[None, :], mixer_query, mixer_forget, mixer_value, mixer_gate,
        expert_tokens, w_gate[0], w_up[0], w_down[0], mixer_proj,
    )
    return pl.pallas_call(
        emit_kernel,
        name="emit",
        out_shape=(shaped(mixer_out.shape, BF16), shaped(expert_out.shape, BF16)),
        in_specs=[any_spec, any_spec],
        out_specs=(any_spec, any_spec),
        scratch_shapes=[dma((2,))],
        compiler_params=pltpu.CompilerParams(vmem_limit_bytes=1000000),
        cost_estimate=cost(1000000, 800000),
    )(mixer_out, expert_out)


def per_device(
    mixer_query, mixer_forget, mixer_value, mixer_gate, forget_floor, head_gain, mixer_proj,
    expert_tokens, expert_gain, routes, group_logits, choice_logits, w_gate, w_up, w_down,
):
    length, width = mixer_query.shape
    heads = width // KEYDIM
    experts = lax.axis_size("ep")
    tp = lax.axis_size("tp")
    rows, model = expert_tokens.shape
    capacity = 2 * TOPK * rows // experts
    slots = experts * capacity
    split = 2
    part = model // split
    which = lax.axis_index("tp") % split
    half = jnp.full((experts + 1,), 0, jnp.int32) + which

    outgoing, wt = pl.pallas_call(
        dispatch_kernel,
        name="dispatch",
        out_shape=(shaped((slots, part), BF16), shaped((2, rows, slots), BF16)),
        in_specs=[SM, VM, VM, VM, VM, VM],
        out_specs=(VM, VM),
        cost_estimate=cost(2 * rows * slots * part, 4000000),
    )(half, expert_tokens, expert_gain[None, :], routes.T, group_logits.T, choice_logits.T)
    arrived = lax.all_to_all(
        outgoing.reshape(experts, capacity, part), "ep", split_axis=0, concat_axis=0, tiled=True
    )

    intra, qexp, pay = pl.pallas_call(
        local_kernel,
        name="local_scan",
        out_shape=(
            shaped((length, width), F32),
            shaped((length, width), BF16),
            shaped((heads, VDIM + PAD, KEYDIM), BF16),
        ),
        in_specs=[VM] * 4,
        out_specs=(VM, VM, VM),
        cost_estimate=cost(3000000000, 4000000),
    )(mixer_query, mixer_forget, mixer_value, forget_floor[None, :])
    arrived, pay = lax.optimization_barrier((arrived, pay))
    entering = prefix(pay, experts)
    mixed = pl.pallas_call(
        finish_kernel,
        name="mixer_finish",
        out_shape=shaped((length, width), BF16),
        in_specs=[VM] * 5,
        out_specs=VM,
        cost_estimate=cost(1000000000, 4000000),
    )(entering, intra, qexp, mixer_gate, head_gain[None, :])
    mixed_all = lax.all_gather(mixed, "tp", axis=1, tiled=True)

    own = arrived.reshape(slots, part)
    other = lax.ppermute(own, "tp", [(i, i ^ 1) for i in range(tp)])
    flat_in = jnp.concatenate(
        [jnp.where(which == 0, own, other), jnp.where(which == 0, other, own)], axis=1
    )
    gate_pre = jnp.dot(flat_in, w_gate[0], preferred_element_type=F32)
    up_pre = jnp.dot(flat_in, w_up[0], preferred_element_type=F32)
    hidden = (jax.nn.silu(gate_pre) * up_pre).astype(BF16)
    hidden_all = lax.all_gather(hidden, "tp", axis=1, tiled=True)
    mixer_out = jnp.dot(mixed_all, mixer_proj, preferred_element_type=F32).astype(BF16)
    down = jnp.dot(hidden_all, w_down[0], preferred_element_type=F32).astype(BF16)
    back = lax.all_to_all(
        down.reshape(experts, capacity, -1), "ep", split_axis=0, concat_axis=0, tiled=True
    ).reshape(slots, -1)
    expert_out = pl.pallas_call(
        return_kernel,
        name="weigh",
        out_shape=shaped((rows, back.shape[1]), BF16),
        in_specs=[VM, VM],
        out_specs=VM,
        cost_estimate=cost(4 * rows * slots * back.shape[1], 1000000),
    )(wt, back)
    return (mixer_out, expert_out)


def solution(mesh):
    paired = mesh.shape["ep"] == GROUPS * TOPK and mesh.shape["tp"] == 4
    return jax.shard_map(
        fused if paired else per_device,
        mesh=mesh,
        in_specs=(
            P("ep", "tp"),
            P("ep", "tp"),
            P("ep", "tp"),
            P("ep", "tp"),
            P("tp"),
            P(),
            P(None, "tp"),
            P("ep", None),
            P(),
            P("ep", None),
            P("ep", None),
            P("ep", None),
            P("ep", None, "tp"),
            P("ep", None, "tp"),
            P("ep", None, "tp"),
        ),
        out_specs=(P("ep", "tp"), P("ep", "tp")),
        check_vma=False,
    )
```

```python
import jax
import jax.numpy as jnp
from jax import lax
from jax.experimental import pallas as pl
from jax.experimental.pallas import tpu as pltpu
from jax.sharding import PartitionSpec as P

KEYDIM = 128
VDIM = 128
GROUPS = 4
TOPK = 2
SPLIT = 2
PAD = 16
norm_eps = 1e-06
F32 = jnp.float32
BF16 = jnp.bfloat16
VM = pl.BlockSpec(memory_space=pltpu.VMEM)
SM = pl.BlockSpec(memory_space=pltpu.SMEM)


def tn_dot(a, b):
    return lax.dot_general(a, b, (((0,), (0,)), ((), ())), preferred_element_type=F32)


def nt_dot(a, b):
    return lax.dot_general(a, b, (((1,), (1,)), ((), ())), preferred_element_type=F32)


def silu(v):
    return v / (1.0 + jnp.exp(-v))


def local_kernel(q_ref, f_ref, v_ref, floor_ref, intra_ref, qexp_ref, pay_ref):
    length = q_ref.shape[0]
    rows = lax.broadcasted_iota(jnp.int32, (length, length), 0)
    cols = lax.broadcasted_iota(jnp.int32, (length, length), 1)
    causal = cols <= rows
    tril = causal.astype(F32)
    for h in range(q_ref.shape[1] // KEYDIM):
        at = slice(h * KEYDIM, (h + 1) * KEYDIM)
        floor = floor_ref[:, at]
        rates = (1.0 - floor) / (1.0 + jnp.exp(f_ref[:, at].astype(F32)))
        cum = jnp.dot(
            tril, jnp.log(1.0 - rates), precision=lax.Precision.HIGHEST,
            preferred_element_type=F32,
        )
        end = cum[length - 1 : length, :]
        qexp = (silu(q_ref[:, at].astype(F32)) * jnp.exp(cum)).astype(BF16)
        kexp = (rates * jnp.exp(-cum)).astype(BF16)
        kend = (rates * jnp.exp(end - cum)).astype(BF16)
        value = v_ref[:, at]
        scores = jnp.where(causal, nt_dot(qexp, kexp), 0.0).astype(BF16)
        intra_ref[:, at] = jnp.dot(scores, value, preferred_element_type=F32)
        qexp_ref[:, at] = qexp
        pay_ref[h, :VDIM, :] = tn_dot(value, kend).astype(BF16)
        pay_ref[h, VDIM:, :] = jnp.broadcast_to(jnp.exp(end), (PAD, KEYDIM)).astype(BF16)


def finish_kernel(state_ref, intra_ref, qexp_ref, gate_ref, gain_ref, out_ref):
    for h in range(intra_ref.shape[1] // VDIM):
        at = slice(h * VDIM, (h + 1) * VDIM)

        out = intra_ref[:, at] + nt_dot(qexp_ref[:, at], state_ref[h, :VDIM, :])
        scale = lax.rsqrt(jnp.mean(out * out, axis=-1, keepdims=True) + norm_eps)
        out_ref[:, at] = (
            out * scale * gain_ref[...] * silu(gate_ref[:, at].astype(F32))
        ).astype(BF16)


def dispatch_kernel(half_ref, x_ref, gain_ref, routes_ref, gl_ref, cl_ref, out_ref, wt_ref):
    rows, width = x_ref.shape
    slots = out_ref.shape[0]
    part = out_ref.shape[1]
    experts = half_ref.shape[0] - 1
    capacity = slots // experts
    group_size = experts // GROUPS
    t0 = lax.broadcasted_iota(jnp.int32, (rows, rows), 0)
    t1 = lax.broadcasted_iota(jnp.int32, (rows, rows), 1)

    def column(row):
        return jnp.sum(jnp.where(t0 == t1, row.astype(F32), 0.0), axis=-1, keepdims=True)

    route = [column(routes_ref[j : j + 1, :]).astype(jnp.int32) for j in range(TOPK)]
    ids = lax.broadcasted_iota(jnp.int32, (rows, experts), 1)
    hot = [(r == ids).astype(F32) for r in route]
    before = jnp.dot(
        (t1 < t0).astype(BF16), sum(hot).astype(BF16), preferred_element_type=F32
    )
    group_exp = [jnp.exp(column(gl_ref[g : g + 1, :])) for g in range(GROUPS)]
    group_sum = sum(group_exp)
    gids = lax.broadcasted_iota(jnp.int32, (rows, GROUPS), 1)
    member = [
        ((r >= gids * group_size) & (r < (gids + 1) * group_size)).astype(F32) for r in route
    ]
    choice = [jnp.exp(column(cl_ref[j : j + 1, :])) for j in range(TOPK)]
    slot_ids = lax.broadcasted_iota(jnp.int32, (rows, slots), 1)
    place = jnp.zeros((rows, slots), F32)
    weight = jnp.zeros((rows, slots), F32)
    for j in range(TOPK):
        rank = jnp.sum(before * hot[j], axis=-1, keepdims=True).astype(jnp.int32)
        mark = (slot_ids == route[j] * capacity + rank).astype(F32)
        within = sum(
            jnp.sum(member[j] * member[i], axis=-1, keepdims=True) * choice[i]
            for i in range(TOPK)
        )
        prob = sum(member[j][:, g : g + 1] * group_exp[g] for g in range(GROUPS)) / group_sum
        place = place + mark
        weight = weight + mark * (prob * choice[j] / within)
    high = weight.astype(BF16)
    wt_ref[0] = high
    wt_ref[1] = (weight - high.astype(F32)).astype(BF16)
    x = x_ref[...].astype(F32)
    scale = lax.rsqrt(jnp.mean(x * x, axis=-1, keepdims=True) + norm_eps)
    cols = pl.ds(pl.multiple_of(half_ref[0] * part, part), part)
    normed = (x_ref[:, cols].astype(F32) * scale * gain_ref[:, cols]).astype(BF16)
    out_ref[...] = tn_dot(place.astype(BF16), normed).astype(BF16)


def return_kernel(wt_ref, back_ref, out_ref):
    back = back_ref[...]
    out_ref[...] = (
        jnp.dot(wt_ref[0], back, preferred_element_type=F32)
        + jnp.dot(wt_ref[1], back, preferred_element_type=F32)
    ).astype(BF16)


def later_after(later, earlier):
    later = later.astype(F32)
    rows = lax.broadcasted_iota(jnp.int32, later.shape, 1)
    decay = later[:, VDIM : VDIM + 1, :]
    return (decay * earlier.astype(F32) + jnp.where(rows < VDIM, later, 0.0)).astype(BF16)


def prefix(pay, count):
    span = pay
    before = None
    step = 1
    while step < count:
        came = lax.ppermute(span, "ep", [(i, i + step) for i in range(count - step)])
        before = came if before is None else later_after(before, came)
        step *= 2
        if step < count:
            span = later_after(span, came)
    return jnp.zeros_like(pay) if before is None else before


def cost(flops, size):
    return pl.CostEstimate(flops=flops, bytes_accessed=size, transcendentals=0)


def shaped(shape, kind):
    return jax.ShapeDtypeStruct(shape, kind)


def remote(src, dst, send, recv, device):
    return pltpu.make_async_remote_copy(
        src_ref=src, dst_ref=dst, send_sem=send, recv_sem=recv, device_id=device,
        device_id_type=pl.DeviceIdType.MESH,
    )


def other_plane(z, k):
    return (z % 2 + k % 2) % 2 + 2 * ((z // 2 + k // 2) % 2)


def split3(v):
    high = v.astype(BF16)
    rest = v - high.astype(F32)
    mid = rest.astype(BF16)
    return high, mid, (rest - mid.astype(F32)).astype(BF16)


def fused_kernel(
    routes_hbm, gl_hbm, cl_hbm, floor_hbm, hgain_hbm, egain_hbm,
    q_hbm, f_hbm, v_hbm, g_hbm, tok_hbm, wg_hbm, wu_hbm, wd_hbm, proj_hbm,
    mixer_ref, expert_ref,
    routes_ref, gl_ref, cl_ref, floor_ref, hgain_ref, egain_ref,
    q_ref, f_ref, v_ref, g_ref, tok_ref, wg_ref, wu_ref, wd_ref, proj_ref,
    disp, wsrc, wgot, flat, hid, vout, vin, ret, back, perm,
    cum_ref, rate_ref, qexp_ref, intra_ref, pay, payin, sums, decays, first, chain_in, chain_out,
    ent, ent_out, mix,
    load_sem, zs, zr, ws, wr, xs, xr, cs, cr, ys, yr, hcs, hcr, vs, vr, rs, rr,
    ps, pr, hs, hr, es, er, ms, mr, mcs, mcr, ds, dr,
):
    ep, tp = lax.axis_index("ep"), lax.axis_index("tp")
    z, x = ep // 2, ep % 2
    y, c = tp // 2, tp % 2
    own = tp
    quarter_y = (1 - y) * 2 + c
    quarter_c = y * 2 + (1 - c)
    quarter_d = (1 - y) * 2 + (1 - c)

    def device(z_, x_, y_, c_):
        return (z_ * 2 + x_, y_ * 2 + c_)

    x_dev = device(z, 1 - x, y, c)
    y_dev = device(z, x, 1 - y, c)
    c_dev = device(z, x, y, 1 - c)
    planes = [other_plane(z, k) for k in range(GROUPS)]
    z_dev = [device(p, x, y, c) for p in planes]

    loads = [
        pltpu.make_async_copy(src, dst, load_sem.at[i])
        for i, (src, dst) in enumerate([
            (routes_hbm, routes_ref), (gl_hbm, gl_ref), (cl_hbm, cl_ref),
            (tok_hbm, tok_ref), (egain_hbm, egain_ref), (floor_hbm, floor_ref), (f_hbm, f_ref), (v_hbm, v_ref), (q_hbm, q_ref),
            (wg_hbm, wg_ref), (wu_hbm, wu_ref), (g_hbm, g_ref), (wd_hbm, wd_ref),
            (proj_hbm, proj_ref), (hgain_hbm, hgain_ref),
        ])
    ]
    (
        routes_load, gl_load, cl_load, tok_load, egain_load, floor_load, f_load, v_load, q_load,
        wg_load, wu_load, g_load, wd_load, proj_load, hgain_load,
    ) = loads
    for load in loads:
        load.start()
    barrier = pltpu.get_barrier_semaphore()
    for dev in z_dev[1:] + [x_dev, y_dev, c_dev]:
        pl.semaphore_signal(
            barrier, inc=1, device_id=dev, device_id_type=pl.DeviceIdType.MESH
        )

    rows = tok_ref.shape[0]
    width = tok_ref.shape[1]
    cap, part = disp.shape[1], disp.shape[2]
    slots = GROUPS * cap
    group_size = TOPK
    routes_load.wait()
    route = [routes_ref[j : j + 1, :] for j in range(TOPK)]
    gids = lax.broadcasted_iota(jnp.int32, (8, rows), 0)
    member = [
        ((r >= gids * group_size) & (r < (gids + 1) * group_size)).astype(F32) for r in route
    ]
    t0 = lax.broadcasted_iota(jnp.int32, (rows, rows), 0)
    t1 = lax.broadcasted_iota(jnp.int32, (rows, rows), 1)
    before = jnp.dot(
        member[0].astype(BF16), (t0 < t1).astype(BF16), preferred_element_type=F32
    )

    def over_groups(v):
        return jnp.sum(v, axis=0, keepdims=True)

    rank = over_groups(before * member[0]).astype(jnp.int32)
    group = over_groups(gids.astype(F32) * member[0]).astype(jnp.int32)
    slot_ids = lax.broadcasted_iota(jnp.int32, (slots, rows), 0)
    perm[...] = (slot_ids == group * cap + rank).astype(F32).astype(BF16)

    tok_load.wait()
    egain_load.wait()
    tokens = tok_ref[...].astype(F32)
    scale = lax.rsqrt(jnp.mean(tokens * tokens, axis=-1, keepdims=True) + norm_eps)
    cols = pl.ds(pl.multiple_of(c * part, part), part)
    normed = (tok_ref[:, cols].astype(F32) * scale * egain_ref[:, cols]).astype(BF16)
    for i in range(GROUPS):
        chosen = perm[i * cap : (i + 1) * cap, :]
        disp[i] = jnp.dot(chosen, normed, preferred_element_type=F32).astype(BF16)
    flat[0, c, x] = disp[z]

    pl.semaphore_wait(barrier, len(z_dev[1:]) + 3)

    half_part = part // 2
    my_cols = pl.ds(pl.multiple_of(y * half_part, half_part), half_part)
    other_cols = pl.ds(pl.multiple_of((1 - y) * half_part, half_part), half_part)
    block = [x, 1 - x]

    def piece(k, b, at=my_cols):
        return flat.at[k, c, b, :, at] if k == SPLIT else flat.at[k, c, b]

    def z_send(k):
        rows_of = disp.at[planes[k], :, my_cols] if k == SPLIT else disp.at[planes[k]]
        return remote(rows_of, piece(k, x), zs.at[k], zr.at[k], z_dev[k])

    def w_send(k):
        return remote(wsrc.at[planes[k]], wgot.at[k], ws.at[k], wr.at[k], z_dev[k])

    def x_send(k, b):
        return remote(piece(k, b), piece(k, b), xs.at[k], xr.at[k], x_dev)

    def d_send(i, at):
        ref = piece(SPLIT, block[i], at)
        return remote(ref, ref, ds.at[i], dr.at[i], y_dev)

    def c_send(k, i, half):
        ref = flat.at[k, half, block[i]]
        return remote(ref, ref, cs.at[k, i], cr.at[k, i], c_dev)

    def arrive_z(k):
        z_send(k).wait_recv()
        x_send(k, x).start()
        if k == SPLIT:
            d_send(0, my_cols).start()
        else:
            c_send(k, 0, c).start()

    def arrive_x(k):
        x_send(k, 1 - x).wait_recv()
        if k == SPLIT:
            d_send(1, my_cols).start()
        else:
            c_send(k, 1, c).start()

    def arrive_d(i):
        d_send(i, other_cols).wait_recv()
        c_send(SPLIT, i, c).start()

    def y_send(k, i, at):
        ref = hid.at[k, block[i], at]
        return remote(ref, ref, ys.at[k, i], yr.at[k, i], y_dev)

    def hc_send(k, i, at, n):
        ref = hid.at[k, block[i], at]
        return remote(ref, ref, hcs.at[k, i, n], hcr.at[k, i, n], c_dev)

    def gate_up(*blocks):
        for k, i in blocks:
            c_send(k, i, 1 - c).wait_recv()
        a = [
            jnp.concatenate([flat[k, n, block[i]] for k, i in blocks], axis=0) for n in range(2)
        ]
        gate = sum(
            jnp.dot(a[n], wg_ref[n * part : (n + 1) * part, :], preferred_element_type=F32)
            for n in range(2)
        )
        up = sum(
            jnp.dot(a[n], wu_ref[n * part : (n + 1) * part, :], preferred_element_type=F32)
            for n in range(2)
        )
        act = (silu(gate) * up).astype(BF16)
        for m, (k, i) in enumerate(blocks):
            hid[k, block[i], own] = act[m * cap : (m + 1) * cap]
            y_send(k, i, own).start()
            hc_send(k, i, own, 0).start()

    def arrive_y(k, i):
        y_send(k, i, quarter_y).wait_recv()
        hc_send(k, i, quarter_y, 1).start()

    depth = wd_ref.shape[0] // 4

    def pieces(k):
        count = 2 if k == GROUPS - 1 else 1
        size = vout.shape[3] // count
        return [slice(j * size, (j + 1) * size) for j in range(count)]

    def v_send(k, j):
        at = pieces(k)[j]
        return remote(vout.at[k, 1, :, at], vin.at[k, :, at], vs.at[k, j], vr.at[k, j], x_dev)

    def down(k):
        for i in range(2):
            hc_send(k, i, quarter_c, 0).wait_recv()
            hc_send(k, i, quarter_d, 1).wait_recv()
        act = [jnp.concatenate([hid[k, block[i], n] for i in range(2)], axis=0) for n in range(4)]
        for j, at in enumerate(pieces(k)):
            value = sum(
                jnp.dot(
                    act[n], wd_ref[n * depth : (n + 1) * depth, at], preferred_element_type=F32
                )
                for n in range(4)
            ).astype(BF16)
            vout[k, 0, :, at] = value[:cap]
            vout[k, 1, :, at] = value[cap:]
            v_send(k, j).start()

    def r_send(k, j):
        at = pieces(k)[j]
        return remote(ret.at[k, :, at], back.at[z, :, at], rs.at[k, j], rr.at[k, j], z_dev[k])

    def combine(k, j=0):
        v_send(k, j).wait_recv()
        if k > 0 and j == 0:
            w_send(k).wait_recv()
        d0 = lax.broadcasted_iota(jnp.int32, (cap, cap), 0)
        d1 = lax.broadcasted_iota(jnp.int32, (cap, cap), 1)
        even, odd = wgot[k, 0:1, :cap], wgot[k, 1:2, :cap]
        mine = jnp.where(x == 0, even, odd)
        theirs = jnp.where(x == 0, odd, even)

        def column(row):
            return jnp.sum(jnp.where(d0 == d1, row, 0.0), axis=-1, keepdims=True)

        at = pieces(k)[j]
        row = (
            column(mine) * vout[k, 0, :, at].astype(F32)
            + column(theirs) * vin[k, :, at].astype(F32)
        ).astype(BF16)
        if k == 0:
            back[z] = row
        else:
            ret[k, :, at] = row
            r_send(k, j).start()

    def weights():
        gl_load.wait()
        cl_load.wait()
        group_exp = [jnp.exp(gl_ref[i : i + 1, :]) for i in range(GROUPS)]
        group_sum = sum(group_exp)
        choice = [jnp.exp(cl_ref[j : j + 1, :]) for j in range(TOPK)]
        expert_weight = [0.0] * group_size
        for j in range(TOPK):
            within = sum(over_groups(member[j] * member[i]) * choice[i] for i in range(TOPK))
            prob = sum(member[j][i : i + 1, :] * group_exp[i] for i in range(GROUPS)) / group_sum
            weight = prob * choice[j] / within
            for m in range(group_size):
                named = route[j] == group * group_size + m
                expert_weight[m] = expert_weight[m] + jnp.where(named, weight, 0.0)
        sub = lax.broadcasted_iota(jnp.int32, (8, rows), 0)
        stacked = jnp.zeros((8, rows), F32)
        for m in range(group_size):
            for i, piece in enumerate(split3(expert_weight[m])):
                stacked = jnp.where(sub == 3 * m + i, piece.astype(F32), stacked)
        stacked = stacked.astype(BF16)
        for i in range(GROUPS):
            chosen = perm[i * cap : (i + 1) * cap, :]
            got = nt_dot(stacked, chosen)
            pair = [got[3 * m : 3 * m + 1, :] + got[3 * m + 1 : 3 * m + 2, :] + got[3 * m + 2 : 3 * m + 3, :]
                    for m in range(group_size)]
            lanes = lax.broadcasted_iota(jnp.int32, (8, cap), 0)
            packed = jnp.where(lanes == 0, pair[0], jnp.where(lanes == 1, pair[1], 0.0))
            wsrc[i] = jnp.concatenate([packed, jnp.zeros((8, wsrc.shape[2] - cap), F32)], axis=1)
        wgot[0] = wsrc[z]
        for k in range(1, GROUPS):
            w_send(k).start()

    length = q_ref.shape[0]
    heads = q_ref.shape[1] // KEYDIM
    lead = heads // 2
    causal = (
        lax.broadcasted_iota(jnp.int32, (length, length), 1)
        <= lax.broadcasted_iota(jnp.int32, (length, length), 0)
    )

    def p_send(start):
        return remote(pay.at[pl.ds(start, lead)], payin, ps, pr, x_dev)

    def payload():
        floor_load.wait()
        f_load.wait()
        v_load.wait()
        tril = causal.astype(F32).astype(BF16)
        rates = (1.0 - floor_ref[...]) / (1.0 + jnp.exp(f_ref[...].astype(F32)))
        rate_ref[...] = rates
        cum = sum(
            jnp.dot(tril, piece, preferred_element_type=F32)
            for piece in split3(jnp.log(1.0 - rates))
        )
        cum_ref[...] = cum
        sub = lax.broadcasted_iota(jnp.int32, (PAD, KEYDIM), 0)
        for h in range(heads):
            at = slice(h * KEYDIM, (h + 1) * KEYDIM)
            end = cum[length - 1 : length, at]
            kend = (rates[:, at] * jnp.exp(end - cum[:, at])).astype(BF16)
            pay[h, :VDIM, :] = tn_dot(v_ref[:, at], kend).astype(BF16)
            high, mid, _ = split3(jnp.exp(end))
            pay[h, VDIM:, :] = jnp.where(
                sub == 0, high.astype(F32), jnp.where(sub == 1, mid.astype(F32), 0.0)
            ).astype(BF16)
        p_send((1 - x) * lead).start()

    def rest(h):
        at = slice(h * KEYDIM, (h + 1) * KEYDIM)
        cum = cum_ref[:, at]
        qexp = (silu(q_ref[:, at].astype(F32)) * jnp.exp(cum)).astype(BF16)
        kexp = (rate_ref[:, at] * jnp.exp(-cum)).astype(BF16)
        scores = jnp.where(causal, nt_dot(qexp, kexp), 0.0).astype(BF16)
        intra_ref[:, at] = jnp.dot(scores, v_ref[:, at], preferred_element_type=F32)
        qexp_ref[:, at] = qexp

    def pair_up():
        p_send(x * lead).wait_recv()
        for i in range(lead):
            mine = pay[x * lead + i].astype(F32)
            theirs = payin[i].astype(F32)
            s0 = jnp.where(x == 0, mine, theirs)
            s1 = jnp.where(x == 0, theirs, mine)
            d0 = s0[VDIM : VDIM + 1, :] + s0[VDIM + 1 : VDIM + 2, :]
            d1 = s1[VDIM : VDIM + 1, :] + s1[VDIM + 1 : VDIM + 2, :]
            sums[i] = d1 * s0[:VDIM, :] + s1[:VDIM, :]
            first[i] = s0[:VDIM, :]
            decays[i, 0:8] = jnp.broadcast_to(d0, (8, KEYDIM))
            decays[i, 8:16] = jnp.broadcast_to(d0 * d1, (8, KEYDIM))

    def h_send():
        return remote(chain_out, chain_in, hs, hr, device((z + 1) % GROUPS, x, y, c))

    def e_send(start):
        return remote(ent_out, ent.at[pl.ds(start, lead)], es, er, x_dev)

    def hop(step):
        @pl.when(z == step)
        def _():
            if step == 0:
                chain_in[...] = jnp.zeros_like(chain_in)
            else:
                h_send().wait_recv()
            if step < GROUPS - 1:
                for i in range(lead):
                    chain_out[i] = (
                        decays[i, 8:9] * chain_in[i].astype(F32) + sums[i]
                    ).astype(BF16)
                h_send().start()
            for i in range(lead):
                came = chain_in[i].astype(F32)
                later = decays[i, 0:1] * came + first[i]
                ent[x * lead + i] = jnp.where(x == 0, came, later).astype(BF16)
                ent_out[i] = jnp.where(x == 0, later, came).astype(BF16)
            e_send(x * lead).start()

    mix_rows = length // 2

    def m_send(j, at):
        ref = mix.at[at, pl.ds(j * mix_rows, mix_rows)]
        return remote(ref, ref, ms.at[j], mr.at[j], y_dev)

    def mc_send(j, at, n):
        ref = mix.at[at, pl.ds(j * mix_rows, mix_rows)]
        return remote(ref, ref, mcs.at[j, n], mcr.at[j, n], c_dev)

    def arrive_ent():
        e_send((1 - x) * lead).wait_recv()

    def finish(j):
        to = slice(j * mix_rows, (j + 1) * mix_rows)
        for h in range(heads):
            at = slice(h * VDIM, (h + 1) * VDIM)
            out = intra_ref[to, at] + nt_dot(qexp_ref[to, at], ent[h])
            norm = lax.rsqrt(jnp.mean(out * out, axis=-1, keepdims=True) + norm_eps)
            mix[own, to, at] = (
                out * norm * hgain_ref[...] * silu(g_ref[to, at].astype(F32))
            ).astype(BF16)
        m_send(j, own).start()
        mc_send(j, own, 0).start()

    def finish_when(ready):
        @pl.when(ready)
        def _():
            arrive_ent()
            finish(0)
            finish(1)

    def arrive_mix(j):
        m_send(j, quarter_y).wait_recv()
        mc_send(j, quarter_y, 1).start()

    def project(j):
        mc_send(j, quarter_c, 0).wait_recv()
        mc_send(j, quarter_d, 1).wait_recv()
        to = slice(j * mix_rows, (j + 1) * mix_rows)
        wide = proj_ref.shape[0] // 4
        mixer_ref[to, :] = sum(
            jnp.dot(mix[i, to, :], proj_ref[i * wide : (i + 1) * wide, :], preferred_element_type=F32)
            for i in range(4)
        ).astype(BF16)

    for k in (2, 1, 3):
        z_send(k).start()
    x_send(0, x).start()
    c_send(0, 0, c).start()
    payload()
    weights()
    q_load.wait()
    rest(0)
    rest(1)
    wg_load.wait()
    wu_load.wait()
    gate_up((0, 0))
    for h in range(2, heads):
        rest(h)
    arrive_z(2)
    arrive_x(0)
    pair_up()
    hop(0)
    arrive_y(0, 0)
    arrive_z(1)
    gate_up((1, 0))
    arrive_d(0)
    arrive_x(2)
    arrive_z(3)
    gate_up((2, 0))
    hop(1)
    arrive_x(1)
    arrive_y(1, 0)
    gate_up((3, 0))
    arrive_d(1)
    gate_up((2, 1), (1, 1))
    wd_load.wait()
    hop(2)
    arrive_x(3)
    arrive_y(2, 0)
    gate_up((3, 1), (0, 1))
    hop(3)
    arrive_y(3, 0)
    g_load.wait()
    hgain_load.wait()
    arrive_y(2, 1)
    finish_when(z < GROUPS - 1)
    arrive_y(1, 1)
    down(2)
    arrive_y(3, 1)
    finish_when(z == GROUPS - 1)
    down(3)
    combine(2)
    arrive_y(0, 1)
    down(1)
    down(0)
    combine(3, 0)
    combine(3, 1)
    combine(1)
    arrive_mix(0)
    combine(0)
    arrive_mix(1)
    proj_load.wait()
    project(0)
    project(1)
    for k in range(1, GROUPS):
        for j in range(len(pieces(k))):
            r_send(k, j).wait_recv()
    expert_ref[...] = tn_dot(perm[...], back[...].reshape(slots, back.shape[2])).astype(BF16)

    for k in range(GROUPS):
        if k > 0:
            z_send(k).wait_send()
            w_send(k).wait_send()
            for j in range(len(pieces(k))):
                r_send(k, j).wait_send()
        x_send(k, x).wait_send()
        for j in range(len(pieces(k))):
            v_send(k, j).wait_send()
        for i in range(2):
            c_send(k, i, c).wait_send()
            y_send(k, i, own).wait_send()
            hc_send(k, i, own, 0).wait_send()
            hc_send(k, i, quarter_y, 1).wait_send()
    for i in range(2):
        d_send(i, my_cols).wait_send()
        m_send(i, own).wait_send()
        mc_send(i, own, 0).wait_send()
        mc_send(i, quarter_y, 1).wait_send()
    p_send((1 - x) * lead).wait_send()
    e_send(x * lead).wait_send()

    @pl.when(z < GROUPS - 1)
    def _():
        h_send().wait_send()


def emit_kernel(mixer_ref, expert_ref, mixer_out, expert_out, sem):
    copies = [
        pltpu.make_async_copy(mixer_ref, mixer_out, sem.at[0]),
        pltpu.make_async_copy(expert_ref, expert_out, sem.at[1]),
    ]
    for copy in copies:
        copy.start()
    for copy in copies:
        copy.wait()


def fused(
    mixer_query, mixer_forget, mixer_value, mixer_gate, forget_floor, head_gain, mixer_proj,
    expert_tokens, expert_gain, routes, group_logits, choice_logits, w_gate, w_up, w_down,
):
    length, width = mixer_query.shape
    heads = width // KEYDIM
    lead = heads // 2
    experts = lax.axis_size("ep")
    rows, model = expert_tokens.shape
    cap = 2 * TOPK * rows // experts
    part = model // 2
    hidden = w_gate.shape[2]
    outs = w_down.shape[2]
    dma, n = pltpu.SemaphoreType.DMA, GROUPS
    any_spec = pl.BlockSpec(memory_space=pl.ANY)
    vmem = pltpu.VMEM
    mixer_out, expert_out = pl.pallas_call(
        fused_kernel,
        name="fused",
        out_shape=(
            vmem((length, mixer_proj.shape[1]), BF16),
            vmem((rows, outs), BF16),
        ),
        in_specs=[any_spec] * 15,
        out_specs=(VM, VM),
        scratch_shapes=[
            vmem((TOPK, rows), jnp.int32), vmem((GROUPS, rows), F32), vmem((TOPK, rows), F32),
            vmem((1, width), F32), vmem((1, VDIM), F32), vmem((1, model), F32),
            vmem((length, width), BF16), vmem((length, width), BF16),
            vmem((length, width), BF16), vmem((length, width), BF16),
            vmem((rows, model), BF16),
            vmem((model, hidden), BF16), vmem((model, hidden), BF16),
            vmem(w_down.shape[1:], BF16), vmem(mixer_proj.shape, BF16),
            vmem((n, cap, part), BF16),
            vmem((n, 8, 128), F32), vmem((n, 8, 128), F32),
            vmem((n, 2, 2, cap, part), BF16),
            vmem((n, 2, 4, cap, hidden), BF16),
            vmem((n, 2, cap, outs), BF16), vmem((n, cap, outs), BF16),
            vmem((n, cap, outs), BF16), vmem((n, cap, outs), BF16),
            vmem((n * cap, rows), BF16),
            vmem((length, width), F32), vmem((length, width), F32),
            vmem((length, width), BF16), vmem((length, width), F32),
            vmem((heads, VDIM + PAD, KEYDIM), BF16), vmem((lead, VDIM + PAD, KEYDIM), BF16),
            vmem((lead, VDIM, KEYDIM), F32), vmem((lead, 16, KEYDIM), F32),
            vmem((lead, VDIM, KEYDIM), F32),
            vmem((lead, VDIM, KEYDIM), BF16), vmem((lead, VDIM, KEYDIM), BF16),
            vmem((heads, VDIM, KEYDIM), BF16), vmem((lead, VDIM, KEYDIM), BF16),
            vmem((4, length, width), BF16),
            dma((15,)), dma((n,)), dma((n,)), dma((n,)), dma((n,)), dma((n,)), dma((n,)),
            dma((n, 2)), dma((n, 2)), dma((n, 2)), dma((n, 2)), dma((n, 2, 2)), dma((n, 2, 2)),
            dma((n, 2)), dma((n, 2)), dma((n, 2)), dma((n, 2)),
            dma, dma, dma, dma, dma, dma, dma((2,)), dma((2,)), dma((2, 2)), dma((2, 2)),
            dma((2,)), dma((2,)),
        ],
        compiler_params=pltpu.CompilerParams(
            collective_id=0, has_side_effects=True, vmem_limit_bytes=64000000
        ),
        cost_estimate=cost(8000000000, 12000000),
    )(
        routes.T, group_logits.T, choice_logits.T, forget_floor[None, :], head_gain[None, :],
        expert_gain[None, :], mixer_query, mixer_forget, mixer_value, mixer_gate,
        expert_tokens, w_gate[0], w_up[0], w_down[0], mixer_proj,
    )
    return pl.pallas_call(
        emit_kernel,
        name="emit",
        out_shape=(shaped(mixer_out.shape, BF16), shaped(expert_out.shape, BF16)),
        in_specs=[any_spec, any_spec],
        out_specs=(any_spec, any_spec),
        scratch_shapes=[dma((2,))],
        compiler_params=pltpu.CompilerParams(vmem_limit_bytes=1000000),
        cost_estimate=cost(1000000, 800000),
    )(mixer_out, expert_out)


def per_device(
    mixer_query, mixer_forget, mixer_value, mixer_gate, forget_floor, head_gain, mixer_proj,
    expert_tokens, expert_gain, routes, group_logits, choice_logits, w_gate, w_up, w_down,
):
    length, width = mixer_query.shape
    heads = width // KEYDIM
    experts = lax.axis_size("ep")
    tp = lax.axis_size("tp")
    rows, model = expert_tokens.shape
    capacity = 2 * TOPK * rows // experts
    slots = experts * capacity
    split = 2
    part = model // split
    which = lax.axis_index("tp") % split
    half = jnp.full((experts + 1,), 0, jnp.int32) + which

    outgoing, wt = pl.pallas_call(
        dispatch_kernel,
        name="dispatch",
        out_shape=(shaped((slots, part), BF16), shaped((2, rows, slots), BF16)),
        in_specs=[SM, VM, VM, VM, VM, VM],
        out_specs=(VM, VM),
        cost_estimate=cost(2 * rows * slots * part, 4000000),
    )(half, expert_tokens, expert_gain[None, :], routes.T, group_logits.T, choice_logits.T)
    arrived = lax.all_to_all(
        outgoing.reshape(experts, capacity, part), "ep", split_axis=0, concat_axis=0, tiled=True
    )

    intra, qexp, pay = pl.pallas_call(
        local_kernel,
        name="local_scan",
        out_shape=(
            shaped((length, width), F32),
            shaped((length, width), BF16),
            shaped((heads, VDIM + PAD, KEYDIM), BF16),
        ),
        in_specs=[VM] * 4,
        out_specs=(VM, VM, VM),
        cost_estimate=cost(3000000000, 4000000),
    )(mixer_query, mixer_forget, mixer_value, forget_floor[None, :])
    arrived, pay = lax.optimization_barrier((arrived, pay))
    entering = prefix(pay, experts)
    mixed = pl.pallas_call(
        finish_kernel,
        name="mixer_finish",
        out_shape=shaped((length, width), BF16),
        in_specs=[VM] * 5,
        out_specs=VM,
        cost_estimate=cost(1000000000, 4000000),
    )(entering, intra, qexp, mixer_gate, head_gain[None, :])
    mixed_all = lax.all_gather(mixed, "tp", axis=1, tiled=True)

    own = arrived.reshape(slots, part)
    other = lax.ppermute(own, "tp", [(i, i ^ 1) for i in range(tp)])
    flat_in = jnp.concatenate(
        [jnp.where(which == 0, own, other), jnp.where(which == 0, other, own)], axis=1
    )
    gate_pre = jnp.dot(flat_in, w_gate[0], preferred_element_type=F32)
    up_pre = jnp.dot(flat_in, w_up[0], preferred_element_type=F32)
    hidden = (jax.nn.silu(gate_pre) * up_pre).astype(BF16)
    hidden_all = lax.all_gather(hidden, "tp", axis=1, tiled=True)
    mixer_out = jnp.dot(mixed_all, mixer_proj, preferred_element_type=F32).astype(BF16)
    down = jnp.dot(hidden_all, w_down[0], preferred_element_type=F32).astype(BF16)
    back = lax.all_to_all(
        down.reshape(experts, capacity, -1), "ep", split_axis=0, concat_axis=0, tiled=True
    ).reshape(slots, -1)
    expert_out = pl.pallas_call(
        return_kernel,
        name="weigh",
        out_shape=shaped((rows, back.shape[1]), BF16),
        in_specs=[VM, VM],
        out_specs=VM,
        cost_estimate=cost(4 * rows * slots * back.shape[1], 1000000),
    )(wt, back)
    return (mixer_out, expert_out)


def solution(mesh):
    paired = mesh.shape["ep"] == GROUPS * TOPK and mesh.shape["tp"] == 4
    return jax.shard_map(
        fused if paired else per_device,
        mesh=mesh,
        in_specs=(
            P("ep", "tp"),
            P("ep", "tp"),
            P("ep", "tp"),
            P("ep", "tp"),
            P("tp"),
            P(),
            P(None, "tp"),
            P("ep", None),
            P(),
            P("ep", None),
            P("ep", None),
            P("ep", None),
            P("ep", None, "tp"),
            P("ep", None, "tp"),
            P("ep", None, "tp"),
        ),
        out_specs=(P("ep", "tp"), P("ep", "tp")),
        check_vma=False,
    )
```
